32 devices in a mesh: sp: 8 (over z, y), tp: 4 (over x, core).
Axes of the slice: x: 2, y: 2, z: 4, core: 2. Of those that a mesh axis runs over, the one named last changes fastest.
Arguments:
- resid: bfloat16 [1024, 2048], P('sp', 'tp'), may hold values from -10.2 to 10.2
- query: bfloat16 [1024, 1024], P('sp', 'tp'), may hold values from -6 to 6
- memory_keys: bfloat16 [1024, 1024], P('sp', 'tp'), may hold values from -6 to 6
- value: bfloat16 [1024, 1024], P('sp', 'tp'), may hold values from -6 to 6
- output_gate_logits: bfloat16 [1024, 1024], P('sp', 'tp'), may hold values from -6 to 6
- gate_preactivation: float32 [4, 8, 1024], P(None, 'tp', 'sp'), may hold values from -6 to 96
- extra_forget_logs: float32 [2, 8, 1024], P(None, 'tp', 'sp'), may hold values from -0.7 to 0
- head_norm_gain: bfloat16 [1024], P('tp'), may hold values from 0.099609375 to 1.8984375
- output_weight: bfloat16 [1024, 2048], P('tp'), may hold values from -0.25 to 0.25
- mixer_norm_gain: bfloat16 [2048], P('tp'), may hold values from 0.099609375 to 1.8984375
- gate_up_weight: bfloat16 [2048, 5632], P('sp', 'tp'), may hold values from -0.125 to 0.125
- value_up_weight: bfloat16 [2048, 5632], P('sp', 'tp'), may hold values from -0.125 to 0.125
- convolution_weight: float32 [3, 5632], P(None, 'tp'), may hold values from -3 to 3
- down_weight: bfloat16 [5632, 2048], P('tp', 'sp'), may hold values from -0.109375 to 0.109375
Outputs:
- out: bfloat16 [1024, 2048], P('sp', 'tp')
The draws below stay inside these ranges and needn't reach their ends.
All inputs are finite; a program needn't handle non-finite values.
Results may differ from the reference program's by a relative error of at most 0.02.
Values may be sent and summed in bfloat16 or wider, within the bound.
A program may use at most 128 MiB of HBM per device.

```python
import jax
import jax.numpy as jnp
from jax import lax

D = 2048
FF = 5632
HEADS = 8
DH = 128
BLOCK = 64
TOK_DEV = 128
SEQ = 1024
CELL_W = 1024
N_TP = 4


def draw_gate_preactivation(key, part):
    keys = jax.random.split(key, 5)
    inputs = jnp.clip(jax.random.normal(keys[0], (2, HEADS, SEQ), jnp.float32), -6.0, 6.0)
    slow_share = 0.5
    jitter = 0.5 * jnp.clip(jax.random.normal(keys[4], (2, HEADS, SEQ), jnp.float32), -4.0, 4.0)
    slow_heads = jax.random.uniform(keys[1], (2, HEADS), jnp.float32) < slow_share
    base_rate = jnp.where(slow_heads, jnp.log(2.0 * SEQ), jnp.log(40.0))
    base_rate = base_rate + jax.random.uniform(keys[2], (2, HEADS), jnp.float32, -0.5, 0.5)
    shard_rate = jax.random.uniform(keys[3], (2, HEADS, SEQ // TOK_DEV), jnp.float32, -0.7, 0.7)
    shard_rate = jnp.repeat(shard_rate, TOK_DEV, axis=2)
    forget = base_rate[..., None] + shard_rate + jitter
    return jnp.stack([inputs[0], forget[0], inputs[1], forget[1]])


def draw_extra_forget_logs(key, part):
    keys = jax.random.split(key, 2)
    positions = jax.random.randint(keys[0], (2, HEADS, 3), 0, SEQ)
    depths = jnp.log(jax.random.uniform(keys[1], (2, HEADS, 3), jnp.float32, 0.5, 0.8))
    places = jnp.arange(SEQ, dtype=jnp.int32)
    matches = (places[None, None, None, :] == positions[..., None]).astype(jnp.float32)
    return jnp.sum(matches * depths[..., None], axis=2)


def draw_resid(key, part):
    keys = jax.random.split(key, 3)
    row_scale = 0.5 * 10.0 ** (0.5 * jax.random.uniform(keys[1], (SEQ, 1), jnp.float32))
    col_scale = 0.16 * 10.0 ** (0.5 * jnp.arange(D, dtype=jnp.float32)[None, :] / D + 0.5 * jax.random.uniform(keys[2], (1, D), jnp.float32))
    jitter = jnp.clip(jax.random.normal(keys[0], (SEQ, D), jnp.float32), -4.0, 4.0)
    return (jitter * row_scale * col_scale).astype(jnp.bfloat16)


def raised(drawn, key, source, target, parts, factor):
    def block_of(position):
        return (jnp.arange(drawn.shape[position]) // (drawn.shape[position] // parts)).reshape((-1,) + (1,) * (drawn.ndim - 1 - position))

    first = jax.random.permutation(key, parts)[block_of(target)]
    other_side = (block_of(target) + parts // 2) % parts
    return jnp.where((block_of(source) == first) | (block_of(source) == other_side), factor * drawn, drawn)


def block_levels(own_key, shape, pieces, low, top_value):
    loudness = 1.0
    for axis_at, shards_of in pieces:
        heights = jax.random.uniform(jax.random.fold_in(jax.random.fold_in(own_key, 6), axis_at), (shards_of,), jnp.float32, low / len(pieces), top_value / len(pieces))
        loudness = loudness * jnp.repeat(jnp.exp(heights), shape[axis_at] // shards_of).reshape((-1,) + (1,) * (len(shape) - 1 - axis_at))
    return loudness


def gaussian(key, shape, width, most, cuts=(), kind=jnp.bfloat16):
    result = width * jax.random.normal(key, shape, jnp.float32)
    if cuts:
        result = result * block_levels(key, shape, cuts, -0.22, 0.18)
    return jnp.clip(result, -most, most).astype(kind)


def gaussian_with(rng, shape, deviation, limit, pieces, heavy, kind=jnp.bfloat16):
    result = deviation * jax.random.normal(rng, shape, jnp.float32)
    if pieces:
        result = result * block_levels(rng, shape, pieces, -0.22, 0.18)
    return jnp.clip(raised(result, jax.random.fold_in(rng, 3), *heavy), -limit, limit).astype(kind)


def setup_inputs(seed: int = 0) -> dict:
    splits = jax.random.split(jax.random.key(seed), 15)
    return {
        "resid": draw_resid(jax.random.fold_in(splits[14], 71), 0),
        "query": gaussian(splits[1], (SEQ, CELL_W), 1.0, 6.0, ((0, 8), (1, 4))),
        "memory_keys": gaussian(splits[2], (SEQ, CELL_W), 1.0, 6.0, ((0, 8), (1, 4))),
        "value": gaussian(splits[3], (SEQ, CELL_W), 1.0, 6.0, ((0, 8), (1, 4))),
        "output_gate_logits": gaussian(splits[4], (SEQ, CELL_W), 1.0, 6.0, ((0, 8), (1, 4))),
        "gate_preactivation": draw_gate_preactivation(jax.random.fold_in(splits[14], 71), 0),
        "extra_forget_logs": draw_extra_forget_logs(jax.random.fold_in(splits[14], 71), 0),
        "head_norm_gain": jnp.clip(1.0 + 0.18 * jax.random.normal(splits[7], (CELL_W,), jnp.float32), 0.099609375, 1.8984375).astype(jnp.bfloat16),
        "output_weight": gaussian_with(splits[8], (CELL_W, D), CELL_W ** -0.5, 0.25, ((0, 4),), (0, 1, 4, 2.0)),
        "mixer_norm_gain": jnp.clip(1.0 + 0.18 * jax.random.normal(splits[9], (D,), jnp.float32), 0.099609375, 1.8984375).astype(jnp.bfloat16),
        "gate_up_weight": gaussian(splits[10], (D, FF), D ** -0.5, 0.125, ((0, 8), (1, 4))),
        "value_up_weight": gaussian(splits[11], (D, FF), D ** -0.5, 0.125, ((0, 8), (1, 4))),
        "convolution_weight": gaussian(splits[12], (3, FF), 1.0, 3.0, ((1, 4),), jnp.float32),
        "down_weight": gaussian_with(splits[13], (FF, D), FF ** -0.5, 0.109375, ((0, 4), (1, 8)), (0, 1, 8, 2.0)),
    }


NEG = -1e+30
EPS = 1e-06
HIGH = lax.Precision.HIGHEST

def heads_blocks(source, head_count):
    length = source.shape[0]
    shaped = source.astype(jnp.float32).reshape(length // BLOCK, BLOCK, head_count, DH)
    return shaped.transpose(2, 0, 1, 3)

def merge_states(earlier, later):
    c_early, m_early, b_early = earlier
    c_late, m_late, b_late = later
    m_new = jnp.maximum(b_late + m_early, m_late)
    c_new = jnp.exp(b_late + m_early - m_new)[..., None, None] * c_early + jnp.exp(m_late - m_new)[..., None, None] * c_late
    return (c_new, m_new, b_early + b_late)

def carry_step(carry, inputs):
    return (merge_states(carry, inputs), carry)

def block_terms(key_rows, values, log_in, log_forget):
    cumulative = jnp.cumsum(log_forget, axis=-1)
    block_end = cumulative[..., -1]
    weight_log = block_end[..., None] - cumulative + log_in
    m_local = lax.optimization_barrier(jnp.max(weight_log, axis=-1))
    weights = jnp.exp(weight_log - m_local[..., None])
    c_local = jnp.einsum('hnsd,hnse->hnde', weights[..., None] * key_rows, values, precision=HIGH)
    return (cumulative, block_end, m_local, c_local)

def block_output(queries, key_rows, values, log_in, cumulative, c_start, m_start):
    a_log = cumulative + m_start[..., None]
    d_log = cumulative[..., :, None] - cumulative[..., None, :] + log_in[..., None, :]
    block_len = cumulative.shape[-1]
    lower_mask = jnp.arange(block_len)[:, None] >= jnp.arange(block_len)[None, :]
    d_log = jnp.where(lower_mask, d_log, -jnp.inf)
    m_row = jnp.maximum(a_log, lax.optimization_barrier(jnp.max(d_log, axis=-1)))
    decays = jnp.exp(d_log - m_row[..., None])
    carried = jnp.exp(a_log - m_row)
    scores = jnp.einsum('hntd,hnsd->hnts', queries, key_rows, precision=HIGH) * decays
    numerator = jnp.einsum('hnts,hnse->hnte', scores, values, precision=HIGH) + carried[..., None] * jnp.einsum('hntd,hnde->hnte', queries, c_start, precision=HIGH)
    return (numerator, m_row)

def single_direction(query, memory_keys, value, log_in, log_forget):
    head_count = query.shape[1] // DH
    nblocks = query.shape[0] // BLOCK
    queries = heads_blocks(query, head_count)
    key_rows = heads_blocks(memory_keys, head_count) * DH ** (-0.5)
    values = heads_blocks(value, head_count)
    log_in = log_in.reshape(head_count, nblocks, BLOCK)
    log_forget = log_forget.reshape(head_count, nblocks, BLOCK)
    cumulative, block_end, m_local, c_local = block_terms(key_rows, values, log_in, log_forget)
    identity = (jnp.zeros((head_count, DH, DH), jnp.float32), jnp.full((head_count,), NEG, jnp.float32), jnp.zeros((head_count,), jnp.float32))
    _, starts = lax.scan(carry_step, identity, (jnp.moveaxis(c_local, 1, 0), m_local.T, block_end.T))
    c_start = jnp.moveaxis(starts[0], 0, 1)
    m_start = starts[1].T
    numerator, m_row = block_output(queries, key_rows, values, log_in, cumulative, c_start, m_start)
    return (numerator.reshape(head_count, -1, DH), m_row.reshape(head_count, -1))

def reference(resid, query, memory_keys, value, output_gate_logits, gate_preactivation, extra_forget_logs, head_norm_gain, output_weight, mixer_norm_gain, gate_up_weight, value_up_weight, convolution_weight, down_weight):
    forward_numerator, forward_peak = single_direction(query, memory_keys, value, gate_preactivation[0], jax.nn.log_sigmoid(gate_preactivation[1]) + extra_forget_logs[0])
    backward_numerator, backward_peak = single_direction(jnp.flip(query, 0), jnp.flip(memory_keys, 0), jnp.flip(value, 0), jnp.flip(gate_preactivation[2], -1), jnp.flip(jax.nn.log_sigmoid(gate_preactivation[3]) + extra_forget_logs[1], -1))
    backward_numerator = jnp.flip(backward_numerator, 1)
    backward_peak = jnp.flip(backward_peak, 1)
    both_max = jnp.maximum(forward_peak, backward_peak)
    numerator = jnp.exp(forward_peak - both_max)[..., None] * forward_numerator + jnp.exp(backward_peak - both_max)[..., None] * backward_numerator
    normal_cell = numerator * lax.rsqrt(lax.optimization_barrier(jnp.mean(numerator * numerator, axis=-1, keepdims=True)) + EPS)
    length = query.shape[0]
    cell = normal_cell.transpose(1, 0, 2).reshape(length, -1)
    cell = (cell * head_norm_gain.astype(jnp.float32) * jax.nn.sigmoid(output_gate_logits.astype(jnp.float32))).astype(jnp.bfloat16)
    group_width = cell.shape[1] // N_TP
    projected = jnp.zeros((length, output_weight.shape[1]), jnp.float32)
    for member in range(N_TP):
        piece = jnp.dot(cell[:, member * group_width:(member + 1) * group_width], output_weight[member * group_width:(member + 1) * group_width], preferred_element_type=jnp.float32)
        projected = projected + lax.optimization_barrier(piece.astype(jnp.bfloat16)).astype(jnp.float32)
    stream = (resid.astype(jnp.float32) + projected).astype(jnp.bfloat16)
    stream_f = stream.astype(jnp.float32)
    normed = (stream_f * lax.rsqrt(lax.optimization_barrier(jnp.mean(stream_f * stream_f, axis=-1, keepdims=True)) + EPS) * mixer_norm_gain.astype(jnp.float32)).astype(jnp.bfloat16)
    gate_mix = jnp.dot(normed, gate_up_weight, preferred_element_type=jnp.float32).astype(jnp.bfloat16)
    value_mix = jnp.dot(normed, value_up_weight, preferred_element_type=jnp.float32).astype(jnp.bfloat16)
    padded_f = jnp.pad(gate_mix.astype(jnp.float32), ((1, 1), (0, 0)))
    conv_taps = convolution_weight.astype(jnp.float32)
    convolved = conv_taps[0] * padded_f[:-2] + conv_taps[1] * padded_f[1:-1] + conv_taps[2] * padded_f[2:]
    hidden = (jax.nn.gelu(convolved) * value_mix.astype(jnp.float32)).astype(jnp.bfloat16)
    unit_width = hidden.shape[1] // N_TP
    mixer_out = jnp.zeros((length, down_weight.shape[1]), jnp.float32)
    for member in range(N_TP):
        piece = jnp.dot(hidden[:, member * unit_width:(member + 1) * unit_width], down_weight[member * unit_width:(member + 1) * unit_width], preferred_element_type=jnp.float32)
        mixer_out = mixer_out + lax.optimization_barrier(piece.astype(jnp.bfloat16)).astype(jnp.float32)
    return (stream_f + mixer_out).astype(jnp.bfloat16)
```

```python
import functools

import jax
import jax.numpy as jnp
from jax import lax
from jax.experimental import pallas as pl
from jax.experimental.pallas import tpu as pltpu
from jax.sharding import PartitionSpec as P

D = 2048
DH = 128
BLOCK = 64


NEG = -1e30
EPS = 1e-06
HIGH = lax.Precision.HIGHEST


def entering(array, axis, combine, identity, reverse):
    size, here = (lax.axis_size(axis), lax.axis_index(axis))
    everything = jax.tree.map(lambda part: lax.all_gather(part, axis), array)
    start = jax.tree.map(
        lambda part, zero: jnp.broadcast_to(jnp.asarray(zero, part.dtype), part.shape),
        array,
        identity,
    )

    def lap(k, before):
        at = size - 1 - k if reverse else k
        reached = at > here if reverse else at < here
        new = combine(before, jax.tree.map(lambda part: part[at], everything))
        return jax.tree.map(lambda a, b: jnp.where(reached, a, b), new, before)

    return lax.fori_loop(0, size, lap, start)


def extended(array, sides, width):
    for axis, dim in sides:
        size, length = (lax.axis_size(axis), array.shape[dim])
        up = [(i, (i + 1) % size) for i in range(size - 1)]
        down = [(j, i) for i, j in up]
        last = lax.slice_in_dim(array, length - width, length, axis=dim)
        first = lax.slice_in_dim(array, 0, width, axis=dim)
        before = lax.ppermute(last, axis, up)
        after = lax.ppermute(first, axis, down)
        array = jnp.concatenate([before, array, after], axis=dim)
    return array


def heads_blocks(source, head_count):
    length = source.shape[0]
    shaped = source.astype(jnp.float32).reshape(length // BLOCK, BLOCK, head_count, DH)
    return shaped.transpose(2, 0, 1, 3)


def merge_states(earlier, later):
    c_early, m_early, b_early = earlier
    c_late, m_late, b_late = later
    m_new = jnp.maximum(b_late + m_early, m_late)
    c_new = (
        jnp.exp(b_late + m_early - m_new)[..., None, None] * c_early
        + jnp.exp(m_late - m_new)[..., None, None] * c_late
    )
    return (c_new, m_new, b_early + b_late)


def carry_step(carry, inputs):
    return (merge_states(carry, inputs), carry)


def block_terms(key_rows, values, log_in, log_forget):
    cumulative = jnp.cumsum(log_forget, axis=-1)
    block_end = cumulative[..., -1]
    weight_log = block_end[..., None] - cumulative + log_in
    m_local = jnp.max(weight_log, axis=-1)
    weights = jnp.exp(weight_log - m_local[..., None])
    c_local = jnp.einsum("hnsd,hnse->hnde", weights[..., None] * key_rows, values, precision=HIGH)
    return (cumulative, block_end, m_local, c_local)


def block_output(queries, key_rows, values, log_in, cumulative, c_start, m_start):
    a_log = cumulative + m_start[..., None]
    d_log = cumulative[..., :, None] - cumulative[..., None, :] + log_in[..., None, :]
    block_len = cumulative.shape[-1]
    lower_mask = jnp.arange(block_len)[:, None] >= jnp.arange(block_len)[None, :]
    d_log = jnp.where(lower_mask, d_log, -jnp.inf)
    m_row = jnp.maximum(a_log, jnp.max(d_log, axis=-1))
    decays = jnp.exp(d_log - m_row[..., None])
    carried = jnp.exp(a_log - m_row)
    scores = jnp.einsum("hntd,hnsd->hnts", queries, key_rows, precision=HIGH) * decays
    numerator = jnp.einsum("hnts,hnse->hnte", scores, values, precision=HIGH) + carried[
        ..., None
    ] * jnp.einsum("hntd,hnde->hnte", queries, c_start, precision=HIGH)
    return (numerator, m_row)


def single_direction(query, memory_keys, value, log_in, log_forget, reverse):
    head_count = query.shape[1] // DH
    nblocks = query.shape[0] // BLOCK
    queries = heads_blocks(query, head_count)
    key_rows = heads_blocks(memory_keys, head_count) * DH ** (-0.5)
    values = heads_blocks(value, head_count)
    log_in = log_in.reshape(head_count, nblocks, BLOCK)
    log_forget = log_forget.reshape(head_count, nblocks, BLOCK)
    cumulative, block_end, m_local, c_local = block_terms(key_rows, values, log_in, log_forget)
    identity = (
        jnp.zeros((head_count, DH, DH), jnp.float32),
        jnp.full((head_count,), NEG, jnp.float32),
        jnp.zeros((head_count,), jnp.float32),
    )
    totals, prefix = lax.scan(
        carry_step, identity, (jnp.moveaxis(c_local, 1, 0), m_local.T, block_end.T)
    )
    if reverse:
        incoming = entering(totals, "sp", merge_states, identity, True)
    else:
        incoming = entering(totals, "sp", merge_states, identity, False)
    starts = merge_states(tuple((member[None] for member in incoming)), prefix)
    c_start = jnp.moveaxis(starts[0], 0, 1)
    m_start = starts[1].T
    numerator, m_row = block_output(queries, key_rows, values, log_in, cumulative, c_start, m_start)
    return (numerator.reshape(head_count, -1, DH), m_row.reshape(head_count, -1))


def per_device(
    resid,
    query,
    memory_keys,
    value,
    output_gate_logits,
    gate_preactivation,
    extra_forget_logs,
    head_norm_gain,
    output_weight,
    mixer_norm_gain,
    gate_up_weight,
    value_up_weight,
    convolution_weight,
    down_weight,
):
    tokens = query.shape[0]
    forward_numerator, forward_peak = single_direction(
        query,
        memory_keys,
        value,
        gate_preactivation[0],
        jax.nn.log_sigmoid(gate_preactivation[1]) + extra_forget_logs[0],
        False,
    )
    backward_numerator, backward_peak = single_direction(
        jnp.flip(query, 0),
        jnp.flip(memory_keys, 0),
        jnp.flip(value, 0),
        jnp.flip(gate_preactivation[2], -1),
        jnp.flip(jax.nn.log_sigmoid(gate_preactivation[3]) + extra_forget_logs[1], -1),
        True,
    )
    backward_numerator = jnp.flip(backward_numerator, 1)
    backward_peak = jnp.flip(backward_peak, 1)
    both_max = jnp.maximum(forward_peak, backward_peak)
    numerator = (
        jnp.exp(forward_peak - both_max)[..., None] * forward_numerator
        + jnp.exp(backward_peak - both_max)[..., None] * backward_numerator
    )
    normal_cell = numerator * lax.rsqrt(
        jnp.mean(numerator * numerator, axis=-1, keepdims=True) + EPS
    )
    cell = normal_cell.transpose(1, 0, 2).reshape(tokens, -1)
    cell = (
        cell
        * head_norm_gain.astype(jnp.float32)
        * jax.nn.sigmoid(output_gate_logits.astype(jnp.float32))
    ).astype(jnp.bfloat16)
    partial_proj = jnp.dot(cell, output_weight, preferred_element_type=jnp.float32)
    stream = (
        resid.astype(jnp.float32)
        + lax.psum_scatter(
            partial_proj.astype(jnp.bfloat16), "tp", scatter_dimension=1, tiled=True
        ).astype(jnp.float32)
    ).astype(jnp.bfloat16)
    stream_f = stream.astype(jnp.float32)
    squares = lax.psum(jnp.sum(stream_f * stream_f, axis=1), "tp")
    normed_own = (
        stream_f * lax.rsqrt(squares / D + EPS)[:, None] * mixer_norm_gain.astype(jnp.float32)
    ).astype(jnp.bfloat16)
    normed = lax.all_gather(normed_own, "tp", axis=1, tiled=True)
    gate_sum = jnp.dot(
        normed,
        lax.all_gather(gate_up_weight, "sp", axis=0, tiled=True),
        preferred_element_type=jnp.float32,
    )
    value_sum = jnp.dot(
        normed,
        lax.all_gather(value_up_weight, "sp", axis=0, tiled=True),
        preferred_element_type=jnp.float32,
    )
    gate_mix = gate_sum.astype(jnp.bfloat16)
    value_mix = value_sum.astype(jnp.bfloat16)
    padded = extended(gate_mix, (("sp", 0),), 1)
    padded_f = padded.astype(jnp.float32)
    convolved = (
        convolution_weight[0] * padded_f[:-2]
        + convolution_weight[1] * padded_f[1:-1]
        + convolution_weight[2] * padded_f[2:]
    )
    hidden = (jax.nn.gelu(convolved) * value_mix.astype(jnp.float32)).astype(jnp.bfloat16)
    down_term = jnp.dot(
        hidden,
        lax.all_gather(down_weight, "sp", axis=1, tiled=True),
        preferred_element_type=jnp.float32,
    )
    mixer_out = lax.psum_scatter(
        down_term.astype(jnp.bfloat16), "tp", scatter_dimension=1, tiled=True
    ).astype(jnp.float32)
    return (stream.astype(jnp.float32) + mixer_out).astype(jnp.bfloat16)


LANE = 128
MESH = pl.DeviceIdType.MESH
F32 = jnp.float32
BF16 = jnp.bfloat16


def remote(src, dst, send, recv, sp, tp):
    return pltpu.make_async_remote_copy(
        src_ref=src,
        dst_ref=dst,
        send_sem=send,
        recv_sem=recv,
        device_id=(sp, tp),
        device_id_type=MESH,
    )


def nt_dot(a, b, precision=None):
    return lax.dot_general(
        a, b, (((1,), (1,)), ((), ())), precision=precision, preferred_element_type=F32
    )


def layer_kernel(
    n_sp,
    n_tp,
    resid,
    query,
    keys,
    value,
    gate_logits,
    gates,
    extra_logs,
    head_gain,
    out_w,
    mixer_gain,
    gate_w,
    value_w,
    taps,
    down_w,
    out,
    k_all,
    v_all,
    g_own,
    g_all,
    lf_own,
    wo_all,
    taps_all,
    gain_own,
    gain_all,
    w_up,
    w_down,
    cell_own,
    cell_all,
    stream_own,
    x_all,
    gate_buf,
    value_buf,
    halo,
    hidden_buf,
    part,
    r_all,
    k_sem,
    v_sem,
    g_sem,
    wo_sem,
    taps_sem,
    gain_sem,
    wg_sem,
    wv_sem,
    wd_sem,
    xg_sem,
    xv_sem,
    xd_sem,
    fwd_sem,
    cell_sem,
    x_send,
    x_recv,
    halo_sem,
    r_send,
    r_recv,
    local_sem,
    local_x,
):
    s, t = (lax.axis_index("sp"), lax.axis_index("tp"))
    core = lax.rem(t, 2)
    pair = t // 2
    partner = t + 1 - 2 * core
    n_pair = n_tp // 2
    tokens = query.shape[0]
    width = query.shape[1]
    features = resid.shape[1]
    depth = gate_w.shape[0]
    cols = down_w.shape[1]
    heads = width // DH
    tiles = gate_w.shape[1] // LANE
    extras = tiles - n_sp
    half = n_sp // 2
    my_half = s // half
    model = features * n_tp

    def loop(low, high, body):
        def step(i, carry):
            body(i)
            return carry

        lax.fori_loop(low, high, step, 0)

    rows = lambda i: pl.ds(pl.multiple_of(i * tokens, tokens), tokens)
    lanes = lambda i, size: pl.ds(pl.multiple_of(i * size, LANE), size)
    drows = lambda i: pl.ds(pl.multiple_of(i * depth, depth), depth)
    trows = lambda i: pl.ds(pl.multiple_of(i * LANE, LANE), LANE)

    def kv_copies(d):
        to = lax.rem(s + d, n_sp)
        return (
            remote(keys, k_all.at[rows(s), :], k_sem.at[0, d], k_sem.at[1, d], to, t),
            remote(value, v_all.at[rows(s), :], v_sem.at[0, d], v_sem.at[1, d], to, t),
        )

    def g_copy(d):
        to = lax.rem(s + d, n_sp)
        return remote(g_own, g_all.at[s], g_sem.at[0, d], g_sem.at[1, d], to, t)

    def wo_copy(e):
        to = lax.rem(t + e, n_tp)
        return remote(
            out_w.at[:, lanes(to, features)],
            wo_all.at[pl.ds(pl.multiple_of(t * width, width), width), :],
            wo_sem.at[0, e],
            wo_sem.at[1, e],
            s,
            to,
        )

    def gain_copy(e):
        to = lax.rem(t + e, n_tp)
        return remote(
            gain_own, gain_all.at[:, lanes(t, features)], gain_sem.at[0, e], gain_sem.at[1, e], s, to
        )

    def taps_copy():
        return remote(taps, taps_all.at[core], taps_sem.at[0], taps_sem.at[1], s, partner)

    def tile_ends(tile, slot):
        return (
            (gate_w.at[:, lanes(tile, LANE)], w_up.at[slot, drows(s), pl.ds(0, LANE)]),
            (value_w.at[:, lanes(tile, LANE)], w_up.at[slot, drows(s), pl.ds(LANE, LANE)]),
            (down_w.at[trows(tile), :], w_down.at[trows(slot), lanes(s, cols)]),
        )

    def weight_copies(d):
        to = lax.rem(s + d, n_sp)
        sems = (wg_sem, wv_sem, wd_sem)
        return tuple(
            remote(a, b, sem.at[0, d], sem.at[1, d], to, t)
            for (a, b), sem in zip(tile_ends(to, core), sems)
        )

    def extra_copies(e, source):
        to = e + extras * core
        sems = (xg_sem, xv_sem, xd_sem)
        return tuple(
            remote(a, b, sem.at[0, e], sem.at[1, source], to, t)
            for (a, b), sem in zip(tile_ends(n_sp + e, 2), sems)
        )

    def local_copies():
        pairs = (
            (keys, k_all.at[rows(s), :]),
            (value, v_all.at[rows(s), :]),
            (out_w.at[:, lanes(t, features)],
             wo_all.at[pl.ds(pl.multiple_of(t * width, width), width), :]),
        ) + tile_ends(s, core)
        return tuple(
            pltpu.make_async_copy(a, b, local_sem.at[i]) for i, (a, b) in enumerate(pairs)
        )

    def local_extra(e):
        return tuple(
            pltpu.make_async_copy(a, b, local_x.at[i])
            for i, (a, b) in enumerate(tile_ends(n_sp + e, 2))
        )

    def start_kv(d):
        for copy in kv_copies(d):
            copy.start()

    loop(1, n_sp, start_kv)
    for copy in local_copies():
        copy.start()

    def log_sigmoid(x):
        return jnp.minimum(x, 0.0) - jnp.log1p(jnp.exp(-jnp.abs(x)))

    lf_own[...] = jnp.zeros_like(lf_own)
    lf_own[0:heads, :] = log_sigmoid(gates[1]) + extra_logs[0]
    lf_own[heads : 2 * heads, :] = log_sigmoid(gates[3]) + extra_logs[1]
    lf = lf_own[...]
    row_id = lax.broadcasted_iota(jnp.int32, (tokens, tokens), 0)
    col_id = lax.broadcasted_iota(jnp.int32, (tokens, tokens), 1)
    upto = (row_id >= col_id).astype(F32)
    below = (row_id > col_id).astype(F32)
    row_incl = nt_dot(lf, upto, HIGH)
    row_excl = nt_dot(lf, below, HIGH)
    col_incl = nt_dot(upto, lf, HIGH)
    col_excl = nt_dot(below, lf, HIGH)
    total = jnp.broadcast_to(jnp.sum(lf, axis=1, keepdims=True), lf.shape)
    g_own[0:heads, :] = gates[0] - row_incl[0:heads]
    g_own[heads : 2 * heads, :] = gates[2] + row_excl[heads : 2 * heads]
    g_own[2 * heads : 4 * heads, :] = total[0 : 2 * heads]
    gain_own[...] = jnp.broadcast_to(mixer_gain[...].astype(F32), gain_own.shape)
    g_all[s] = g_own[...]
    gain_all[:, lanes(t, features)] = gain_own[...]
    taps_all[core] = taps[...]
    loop(1, n_sp, lambda d: g_copy(d).start())

    def start_tp(e):
        wo_copy(e).start()
        gain_copy(e).start()

    loop(1, n_tp, start_tp)
    taps_copy().start()

    def start_weights(d):
        for copy in weight_copies(d):
            copy.start()

    loop(1, n_sp, start_weights)

    def start_extra(e):
        @pl.when(e + extras * core != s)
        def _():
            for copy in extra_copies(e, s):
                copy.start()

        @pl.when(e + extras * core == s)
        def _():
            for copy in local_extra(e):
                copy.start()

    loop(0, extras, start_extra)

    loop(1, n_sp, lambda d: g_copy(d).wait_recv())

    def wait_kv(d):
        for copy in kv_copies(d):
            copy.wait_recv()

    for copy in local_copies()[:3]:
        copy.wait()
    g = [g_all[j] for j in range(n_sp)]
    diag_lower = row_id >= col_id
    diag_upper = row_id <= col_id
    logs, peaks = ([], [])
    for h in range(heads):
        acc = jnp.zeros((1, tokens), F32)
        rows_f = [None] * n_sp
        for j in reversed(range(n_sp)):
            acc = acc + jnp.where(j < s, g[j][2 * heads + h : 2 * heads + h + 1], 0.0)
            rows_f[j] = g[j][h : h + 1] + acc
        acc = jnp.zeros((1, tokens), F32)
        logs_h = []
        f_col = col_incl[:, h : h + 1]
        b_col = -col_excl[:, heads + h : heads + h + 1]
        peak = jnp.full((tokens, 1), NEG, F32)
        for j in range(n_sp):
            row_b = g[j][heads + h : heads + h + 1] + acc
            acc = acc + jnp.where(j >= s, g[j][3 * heads + h : 3 * heads + h + 1], 0.0)
            fwd = jnp.where(jnp.logical_or(j < s, jnp.logical_and(j == s, diag_lower)), f_col + rows_f[j], NEG)
            bwd = jnp.where(jnp.logical_or(j > s, jnp.logical_and(j == s, diag_upper)), b_col + row_b, NEG)
            peak = jnp.maximum(peak, jnp.max(jnp.maximum(fwd, bwd), axis=1, keepdims=True))
            logs_h.append((fwd, bwd))
        peaks.append(peak)
        logs.append(
            jnp.concatenate([jnp.exp(f - peak) + jnp.exp(b - peak) for f, b in logs_h], axis=1)
        )
    loop(1, n_sp, wait_kv)
    for h in range(heads):
        lane = slice(h * DH, (h + 1) * DH)
        scores = nt_dot(query[:, lane], k_all[:, lane]) * DH ** (-0.5)
        weighted = (scores * logs[h]).astype(BF16)
        numer = jnp.dot(weighted, v_all[:, lane], preferred_element_type=F32)
        scale = lax.rsqrt(jnp.mean(numer * numer, axis=1, keepdims=True) + EPS)
        gated = (
            numer * scale * head_gain[:, lane].astype(F32)
            * jax.nn.sigmoid(gate_logits[:, lane].astype(F32))
        )
        cell_own[:, lane] = gated.astype(BF16)

    def cell_copy(e):
        to = lax.rem(t + e, n_tp)
        return remote(cell_own, cell_all.at[t], cell_sem.at[0, e], cell_sem.at[1, e], s, to)

    loop(1, n_tp, lambda e: cell_copy(e).start())
    cell_all[t] = cell_own[...]

    def wait_tp(e):
        wo_copy(e).wait_recv()
        gain_copy(e).wait_recv()
        cell_copy(e).wait_recv()

    loop(1, n_tp, wait_tp)
    projected = jnp.zeros((tokens, features), F32)
    for m in range(n_tp):
        piece = jnp.dot(
            cell_all[m], wo_all[m * width : (m + 1) * width, :], preferred_element_type=F32
        )
        projected = projected + piece.astype(BF16).astype(F32)
    stream_own[...] = (resid[...].astype(F32) + projected).astype(BF16)

    place = lax.rem(s, half)

    def x_copy(d):
        chip = lax.rem(s * n_pair + pair + d, n_sp * n_pair)
        to_s, to_t = (chip // n_pair, 2 * lax.rem(chip, n_pair) + my_half)
        return to_s, to_t, remote(
            stream_own,
            x_all.at[place, :, lanes(t, features)],
            x_send.at[d],
            x_recv.at[place * n_tp + t],
            to_s,
            to_t,
        )

    def start_x(d):
        to_s, to_t, copy = x_copy(d)
        mine = jnp.logical_and(to_s == s, to_t == t)

        @pl.when(jnp.logical_not(mine))
        def _():
            copy.start()

        @pl.when(mine)
        def _():
            x_all[place, :, lanes(t, features)] = stream_own[...]

    loop(0, n_sp * n_pair, start_x)

    def wait_weights(d):
        for copy in weight_copies(d):
            copy.wait_recv()

    loop(1, n_sp, wait_weights)
    for copy in local_copies()[3:]:
        copy.wait()
    owner = jnp.logical_and(s >= extras * core, s < extras * (core + 1))
    other_owner = jnp.logical_and(s >= extras * (1 - core), s < extras * (2 - core))

    def forward_copies(slot, base):
        return (
            remote(w_up.at[slot], w_up.at[slot], fwd_sem.at[0, base], fwd_sem.at[1, base], s, partner),
            remote(
                w_down.at[trows(slot), :],
                w_down.at[trows(slot), :],
                fwd_sem.at[0, base + 1],
                fwd_sem.at[1, base + 1],
                s,
                partner,
            ),
        )

    for copy in forward_copies(core, 0):
        copy.start()

    @pl.when(owner)
    def _():
        def wait_extra(source):
            @pl.when(source != s)
            def _():
                for copy in extra_copies(0, source):
                    copy.wait_recv()

        loop(0, n_sp, wait_extra)
        for copy in local_extra(0):
            copy.wait()
        for copy in forward_copies(2, 2):
            copy.start()

    @pl.when(s >= 2 * extras)
    def _():
        w_up[2] = jnp.zeros(w_up.shape[1:], BF16)
        w_down[2 * LANE :, :] = jnp.zeros((LANE, w_down.shape[1]), BF16)

    taps_copy().wait_recv()
    for copy in forward_copies(1 - core, 0):
        copy.wait_recv()

    @pl.when(other_owner)
    def _():
        for copy in forward_copies(2, 2):
            copy.wait_recv()

    def mix_block(j):
        for m in range(n_tp):
            mine = jnp.logical_and(core * half + j == s, t == m)

            @pl.when(jnp.logical_not(mine))
            def _(m=m):
                remote(
                    stream_own,
                    x_all.at[j, :, pl.ds(m * features, features)],
                    x_send.at[0],
                    x_recv.at[j * n_tp + m],
                    s,
                    partner,
                ).wait_recv()

        x = x_all[j].astype(F32)
        squares = jnp.sum(x * x, axis=1, keepdims=True)
        normed = (x * lax.rsqrt(squares / model + EPS) * gain_all[0:1, :]).astype(BF16)
        for slot in range(3):
            both = jnp.dot(normed, w_up[slot], preferred_element_type=F32).astype(BF16)
            lane = slice(slot * LANE, (slot + 1) * LANE)
            gate_buf[rows(j), lane] = both[:, :LANE]
            value_buf[rows(j), lane] = both[:, LANE:]

    loop(0, half, mix_block)

    count = half * tokens
    edge = halo.shape[0]

    def halo_copy():
        start = pl.multiple_of((1 - core) * (count - edge), edge)
        return remote(
            gate_buf.at[pl.ds(start, edge), :], halo, halo_sem.at[0], halo_sem.at[1], s, partner
        )

    halo_copy().start()
    halo_copy().wait_recv()
    extra_core = jnp.where(s < extras, 0, 1)
    extra_tile = jnp.minimum(n_sp + s - extras * extra_core, tiles - 1)
    slots = ((0, s), (1, s), (extra_core, extra_tile))
    pos = lax.broadcasted_iota(jnp.int32, (count, LANE), 0)
    for slot, (block, tile) in enumerate(slots):
        lane = slice(slot * LANE, (slot + 1) * LANE)
        tap = taps_all[block, :, lanes(tile, LANE)]
        g_mid = gate_buf[:, lane].astype(F32)
        edge_rows = halo[:, lane].astype(F32)
        before = jnp.where(core == 1, edge_rows[edge - 1 : edge], 0.0)
        after = jnp.where(core == 0, edge_rows[0:1], 0.0)
        g_prev = jnp.where(pos == 0, before, pltpu.roll(g_mid, 1, 0))
        g_next = jnp.where(pos == count - 1, after, pltpu.roll(g_mid, count - 1, 0))
        conv = tap[0:1] * g_prev + tap[1:2] * g_mid + tap[2:3] * g_next
        mixed = jax.nn.gelu(conv) * value_buf[:, lane].astype(F32)
        hidden_buf[:, lane] = mixed.astype(BF16)

    chip_id = s * n_pair + pair

    def r_copy(i):
        j, m = (i // n_tp, lax.rem(i, n_tp))
        return j, m, remote(
            part.at[i], r_all.at[chip_id], r_send.at[i], r_recv.at[chip_id], core * half + j, m
        )

    def r_index(i):
        return lax.rem(i + chip_id, half * n_tp)

    def down_block(k):
        i = r_index(k)
        j, m, copy = r_copy(i)
        result = jnp.dot(
            hidden_buf[rows(j), :], w_down[:, lanes(m, features)], preferred_element_type=F32
        ).astype(BF16)
        part[i] = result
        mine = jnp.logical_and(core * half + j == s, m == t)

        @pl.when(jnp.logical_not(mine))
        def _():
            copy.start()

        @pl.when(mine)
        def _():
            r_all[chip_id] = result

    loop(0, half * n_tp, down_block)

    out_sum = jnp.zeros((tokens, features), F32)
    own_core = core == my_half
    for i in range(n_sp * n_pair):
        mine = jnp.logical_and(own_core, chip_id == i)

        @pl.when(jnp.logical_not(mine))
        def _(i=i):
            remote(part.at[0], r_all.at[i], r_send.at[0], r_recv.at[i], s, partner).wait_recv()

        out_sum = out_sum + r_all[i].astype(F32)
    out[...] = (stream_own[...].astype(F32) + out_sum).astype(BF16)

    def sent_sp(d):
        for copy in kv_copies(d) + (g_copy(d),) + weight_copies(d):
            copy.wait_send()

    loop(1, n_sp, sent_sp)

    def sent_tp(e):
        wo_copy(e).wait_send()
        gain_copy(e).wait_send()
        cell_copy(e).wait_send()

    loop(1, n_tp, sent_tp)
    taps_copy().wait_send()

    def sent_extra(e):
        @pl.when(e + extras * core != s)
        def _():
            for copy in extra_copies(e, s):
                copy.wait_send()

    loop(0, extras, sent_extra)

    def sent_x(d):
        to_s, to_t, copy = x_copy(d)

        @pl.when(jnp.logical_not(jnp.logical_and(to_s == s, to_t == t)))
        def _():
            copy.wait_send()

    loop(0, n_sp * n_pair, sent_x)
    for copy in forward_copies(core, 0):
        copy.wait_send()

    @pl.when(owner)
    def _():
        for copy in forward_copies(2, 2):
            copy.wait_send()

    halo_copy().wait_send()

    def sent_r(i):
        j, m, copy = r_copy(i)

        @pl.when(jnp.logical_not(jnp.logical_and(core * half + j == s, m == t)))
        def _():
            copy.wait_send()

    loop(0, half * n_tp, sent_r)


def fast_layer(n_sp, n_tp, *args):
    (resid, query, keys, value, gate_logits, gates, extra_logs, head_gain, out_w,
     mixer_gain, gate_w, value_w, taps, down_w) = args
    tokens, width = query.shape
    features = resid.shape[1]
    model = features * n_tp
    half = n_sp // 2
    n_pair = n_tp // 2
    hidden = 3 * LANE
    vmem = pl.BlockSpec(memory_space=pltpu.VMEM)
    anywhere = pl.BlockSpec(memory_space=pl.ANY)
    dma = pltpu.SemaphoreType.DMA
    spaces = [vmem, vmem, anywhere, anywhere, vmem, vmem, vmem, vmem, anywhere,
              vmem, anywhere, anywhere, vmem, anywhere]
    scratch = [
        pltpu.VMEM((n_sp * tokens, width), BF16),
        pltpu.VMEM((n_sp * tokens, width), BF16),
        pltpu.VMEM((8, tokens), F32),
        pltpu.VMEM((n_sp, 8, tokens), F32),
        pltpu.VMEM((8, tokens), F32),
        pltpu.VMEM((n_tp * width, features), BF16),
        pltpu.VMEM((2,) + taps.shape, F32),
        pltpu.VMEM((8, features), F32),
        pltpu.VMEM((8, model), F32),
        pltpu.VMEM((3, model, 2 * LANE), BF16),
        pltpu.VMEM((hidden, model), BF16),
        pltpu.VMEM((tokens, width), BF16),
        pltpu.VMEM((n_tp, tokens, width), BF16),
        pltpu.VMEM((tokens, features), BF16),
        pltpu.VMEM((half, tokens, model), BF16),
        pltpu.VMEM((half * tokens, hidden), BF16),
        pltpu.VMEM((half * tokens, hidden), BF16),
        pltpu.VMEM((16, hidden), BF16),
        pltpu.VMEM((half * tokens, hidden), BF16),
        pltpu.VMEM((half * n_tp, tokens, features), BF16),
        pltpu.VMEM((n_sp * n_pair, tokens, features), BF16),
        dma((2, n_sp)),
        dma((2, n_sp)),
        dma((2, n_sp)),
        dma((2, n_tp)),
        dma((2,)),
        dma((2, n_tp)),
        dma((2, n_sp)),
        dma((2, n_sp)),
        dma((2, n_sp)),
        dma((2, n_sp)),
        dma((2, n_sp)),
        dma((2, n_sp)),
        dma((2, 4)),
        dma((2, n_tp)),
        dma((n_sp * n_pair,)),
        dma((half * n_tp,)),
        dma((2,)),
        dma((half * n_tp,)),
        dma((n_sp * n_pair,)),
        dma((6,)),
        dma((3,)),
    ]
    return pl.pallas_call(
        functools.partial(layer_kernel, n_sp, n_tp),
        out_shape=jax.ShapeDtypeStruct((tokens, features), BF16),
        in_specs=spaces,
        out_specs=vmem,
        scratch_shapes=scratch,
        compiler_params=pltpu.CompilerParams(has_side_effects=True, vmem_limit_bytes=60 * 2**20),
    )(resid, query, keys, value, gate_logits, gates, extra_logs, head_gain.reshape(1, -1), out_w,
      mixer_gain.reshape(1, -1), gate_w, value_w, taps, down_w)


def choose(n_sp, n_tp, *args):
    tokens, width = args[1].shape
    tiles, rest = divmod(args[10].shape[1], LANE)
    fits = (
        n_sp % 2 == 0
        and n_tp % 2 == 0
        and rest == 0
        and 0 < tiles - n_sp
        and 2 * (tiles - n_sp) <= n_sp
        and tokens == LANE
        and width == 2 * DH
        and n_sp * tokens <= 1024
    )
    if fits:
        return fast_layer(n_sp, n_tp, *args)
    return per_device(*args)


def solution(mesh):
    return jax.shard_map(
        functools.partial(choose, mesh.shape["sp"], mesh.shape["tp"]),
        mesh=mesh,
        in_specs=(
            P("sp", "tp"),
            P("sp", "tp"),
            P("sp", "tp"),
            P("sp", "tp"),
            P("sp", "tp"),
            P(None, "tp", "sp"),
            P(None, "tp", "sp"),
            P("tp"),
            P("tp", None),
            P("tp"),
            P("sp", "tp"),
            P("sp", "tp"),
            P(None, "tp"),
            P("tp", "sp"),
        ),
        out_specs=P("sp", "tp"),
        check_vma=False,
    )
```

```python
import functools

import jax
import jax.numpy as jnp
from jax import lax
from jax.experimental import pallas as pl
from jax.experimental.pallas import tpu as pltpu
from jax.sharding import PartitionSpec as P

D = 2048
DH = 128
BLOCK = 64


NEG = -1e30
EPS = 1e-06
HIGH = lax.Precision.HIGHEST


def entering(array, axis, combine, identity, reverse):
    size, here = (lax.axis_size(axis), lax.axis_index(axis))
    everything = jax.tree.map(lambda part: lax.all_gather(part, axis), array)
    start = jax.tree.map(
        lambda part, zero: jnp.broadcast_to(jnp.asarray(zero, part.dtype), part.shape),
        array,
        identity,
    )

    def lap(k, before):
        at = size - 1 - k if reverse else k
        reached = at > here if reverse else at < here
        new = combine(before, jax.tree.map(lambda part: part[at], everything))
        return jax.tree.map(lambda a, b: jnp.where(reached, a, b), new, before)

    return lax.fori_loop(0, size, lap, start)


def extended(array, sides, width):
    for axis, dim in sides:
        size, length = (lax.axis_size(axis), array.shape[dim])
        up = [(i, (i + 1) % size) for i in range(size - 1)]
        down = [(j, i) for i, j in up]
        last = lax.slice_in_dim(array, length - width, length, axis=dim)
        first = lax.slice_in_dim(array, 0, width, axis=dim)
        before = lax.ppermute(last, axis, up)
        after = lax.ppermute(first, axis, down)
        array = jnp.concatenate([before, array, after], axis=dim)
    return array


def heads_blocks(source, head_count):
    length = source.shape[0]
    shaped = source.astype(jnp.float32).reshape(length // BLOCK, BLOCK, head_count, DH)
    return shaped.transpose(2, 0, 1, 3)


def merge_states(earlier, later):
    c_early, m_early, b_early = earlier
    c_late, m_late, b_late = later
    m_new = jnp.maximum(b_late + m_early, m_late)
    c_new = (
        jnp.exp(b_late + m_early - m_new)[..., None, None] * c_early
        + jnp.exp(m_late - m_new)[..., None, None] * c_late
    )
    return (c_new, m_new, b_early + b_late)


def carry_step(carry, inputs):
    return (merge_states(carry, inputs), carry)


def block_terms(key_rows, values, log_in, log_forget):
    cumulative = jnp.cumsum(log_forget, axis=-1)
    block_end = cumulative[..., -1]
    weight_log = block_end[..., None] - cumulative + log_in
    m_local = jnp.max(weight_log, axis=-1)
    weights = jnp.exp(weight_log - m_local[..., None])
    c_local = jnp.einsum("hnsd,hnse->hnde", weights[..., None] * key_rows, values, precision=HIGH)
    return (cumulative, block_end, m_local, c_local)


def block_output(queries, key_rows, values, log_in, cumulative, c_start, m_start):
    a_log = cumulative + m_start[..., None]
    d_log = cumulative[..., :, None] - cumulative[..., None, :] + log_in[..., None, :]
    block_len = cumulative.shape[-1]
    lower_mask = jnp.arange(block_len)[:, None] >= jnp.arange(block_len)[None, :]
    d_log = jnp.where(lower_mask, d_log, -jnp.inf)
    m_row = jnp.maximum(a_log, jnp.max(d_log, axis=-1))
    decays = jnp.exp(d_log - m_row[..., None])
    carried = jnp.exp(a_log - m_row)
    scores = jnp.einsum("hntd,hnsd->hnts", queries, key_rows, precision=HIGH) * decays
    numerator = jnp.einsum("hnts,hnse->hnte", scores, values, precision=HIGH) + carried[
        ..., None
    ] * jnp.einsum("hntd,hnde->hnte", queries, c_start, precision=HIGH)
    return (numerator, m_row)


def single_direction(query, memory_keys, value, log_in, log_forget, reverse):
    head_count = query.shape[1] // DH
    nblocks = query.shape[0] // BLOCK
    queries = heads_blocks(query, head_count)
    key_rows = heads_blocks(memory_keys, head_count) * DH ** (-0.5)
    values = heads_blocks(value, head_count)
    log_in = log_in.reshape(head_count, nblocks, BLOCK)
    log_forget = log_forget.reshape(head_count, nblocks, BLOCK)
    cumulative, block_end, m_local, c_local = block_terms(key_rows, values, log_in, log_forget)
    identity = (
        jnp.zeros((head_count, DH, DH), jnp.float32),
        jnp.full((head_count,), NEG, jnp.float32),
        jnp.zeros((head_count,), jnp.float32),
    )
    totals, prefix = lax.scan(
        carry_step, identity, (jnp.moveaxis(c_local, 1, 0), m_local.T, block_end.T)
    )
    if reverse:
        incoming = entering(totals, "sp", merge_states, identity, True)
    else:
        incoming = entering(totals, "sp", merge_states, identity, False)
    starts = merge_states(tuple((member[None] for member in incoming)), prefix)
    c_start = jnp.moveaxis(starts[0], 0, 1)
    m_start = starts[1].T
    numerator, m_row = block_output(queries, key_rows, values, log_in, cumulative, c_start, m_start)
    return (numerator.reshape(head_count, -1, DH), m_row.reshape(head_count, -1))


def per_device(
    resid,
    query,
    memory_keys,
    value,
    output_gate_logits,
    gate_preactivation,
    extra_forget_logs,
    head_norm_gain,
    output_weight,
    mixer_norm_gain,
    gate_up_weight,
    value_up_weight,
    convolution_weight,
    down_weight,
):
    tokens = query.shape[0]
    forward_numerator, forward_peak = single_direction(
        query,
        memory_keys,
        value,
        gate_preactivation[0],
        jax.nn.log_sigmoid(gate_preactivation[1]) + extra_forget_logs[0],
        False,
    )
    backward_numerator, backward_peak = single_direction(
        jnp.flip(query, 0),
        jnp.flip(memory_keys, 0),
        jnp.flip(value, 0),
        jnp.flip(gate_preactivation[2], -1),
        jnp.flip(jax.nn.log_sigmoid(gate_preactivation[3]) + extra_forget_logs[1], -1),
        True,
    )
    backward_numerator = jnp.flip(backward_numerator, 1)
    backward_peak = jnp.flip(backward_peak, 1)
    both_max = jnp.maximum(forward_peak, backward_peak)
    numerator = (
        jnp.exp(forward_peak - both_max)[..., None] * forward_numerator
        + jnp.exp(backward_peak - both_max)[..., None] * backward_numerator
    )
    normal_cell = numerator * lax.rsqrt(
        jnp.mean(numerator * numerator, axis=-1, keepdims=True) + EPS
    )
    cell = normal_cell.transpose(1, 0, 2).reshape(tokens, -1)
    cell = (
        cell
        * head_norm_gain.astype(jnp.float32)
        * jax.nn.sigmoid(output_gate_logits.astype(jnp.float32))
    ).astype(jnp.bfloat16)
    partial_proj = jnp.dot(cell, output_weight, preferred_element_type=jnp.float32)
    stream = (
        resid.astype(jnp.float32)
        + lax.psum_scatter(
            partial_proj.astype(jnp.bfloat16), "tp", scatter_dimension=1, tiled=True
        ).astype(jnp.float32)
    ).astype(jnp.bfloat16)
    stream_f = stream.astype(jnp.float32)
    squares = lax.psum(jnp.sum(stream_f * stream_f, axis=1), "tp")
    normed_own = (
        stream_f * lax.rsqrt(squares / D + EPS)[:, None] * mixer_norm_gain.astype(jnp.float32)
    ).astype(jnp.bfloat16)
    normed = lax.all_gather(normed_own, "tp", axis=1, tiled=True)
    gate_sum = jnp.dot(
        normed,
        lax.all_gather(gate_up_weight, "sp", axis=0, tiled=True),
        preferred_element_type=jnp.float32,
    )
    value_sum = jnp.dot(
        normed,
        lax.all_gather(value_up_weight, "sp", axis=0, tiled=True),
        preferred_element_type=jnp.float32,
    )
    gate_mix = gate_sum.astype(jnp.bfloat16)
    value_mix = value_sum.astype(jnp.bfloat16)
    padded = extended(gate_mix, (("sp", 0),), 1)
    padded_f = padded.astype(jnp.float32)
    convolved = (
        convolution_weight[0] * padded_f[:-2]
        + convolution_weight[1] * padded_f[1:-1]
        + convolution_weight[2] * padded_f[2:]
    )
    hidden = (jax.nn.gelu(convolved) * value_mix.astype(jnp.float32)).astype(jnp.bfloat16)
    down_term = jnp.dot(
        hidden,
        lax.all_gather(down_weight, "sp", axis=1, tiled=True),
        preferred_element_type=jnp.float32,
    )
    mixer_out = lax.psum_scatter(
        down_term.astype(jnp.bfloat16), "tp", scatter_dimension=1, tiled=True
    ).astype(jnp.float32)
    return (stream.astype(jnp.float32) + mixer_out).astype(jnp.bfloat16)


LANE = 128
MESH = pl.DeviceIdType.MESH
F32 = jnp.float32
BF16 = jnp.bfloat16


def remote(src, dst, send, recv, sp, tp):
    return pltpu.make_async_remote_copy(
        src_ref=src,
        dst_ref=dst,
        send_sem=send,
        recv_sem=recv,
        device_id=(sp, tp),
        device_id_type=MESH,
    )


def nt_dot(a, b, precision=None):
    return lax.dot_general(
        a, b, (((1,), (1,)), ((), ())), precision=precision, preferred_element_type=F32
    )


def layer_kernel(
    n_sp,
    n_tp,
    resid,
    query,
    keys,
    value,
    gate_logits,
    gates,
    extra_logs,
    head_gain,
    out_w,
    mixer_gain,
    gate_w,
    value_w,
    taps,
    down_w,
    out,
    k_all,
    v_all,
    g_own,
    g_all,
    lf_own,
    wo_all,
    taps_all,
    gain_own,
    gain_all,
    w_up,
    w_down,
    cell_own,
    cell_all,
    stream_own,
    x_all,
    gate_buf,
    value_buf,
    halo,
    hidden_buf,
    part,
    part_sum,
    part_in,
    sum_in,
    z_out,
    r_all,
    k_sem,
    v_sem,
    g_sem,
    wo_sem,
    taps_sem,
    gain_sem,
    wg_sem,
    wv_sem,
    wd_sem,
    xg_sem,
    xv_sem,
    xd_sem,
    fwd_sem,
    cell_sem,
    x_send,
    x_fwd,
    x_relay,
    x_recv,
    halo_sem,
    p_sem,
    q_sem,
    z_send,
    r_recv,
    local_sem,
    local_x,
):
    s, t = (lax.axis_index("sp"), lax.axis_index("tp"))
    core = lax.rem(t, 2)
    pair = t // 2
    partner = t + 1 - 2 * core
    n_pair = n_tp // 2
    tokens = query.shape[0]
    width = query.shape[1]
    features = resid.shape[1]
    depth = gate_w.shape[0]
    cols = down_w.shape[1]
    heads = width // DH
    tiles = gate_w.shape[1] // LANE
    extras = tiles - n_sp
    half = n_sp // 2
    my_half = s // half
    model = features * n_tp
    z, y = (s // 2, lax.rem(s, 2))
    layers = half // 2
    x_side = (s, 2 * (1 - pair) + core)
    y_side = (2 * z + 1 - y, t)

    def loop(low, high, body):
        def step(i, carry):
            body(i)
            return carry

        lax.fori_loop(low, high, step, 0)

    rows = lambda i: pl.ds(pl.multiple_of(i * tokens, tokens), tokens)
    lanes = lambda i, size: pl.ds(pl.multiple_of(i * size, LANE), size)
    drows = lambda i: pl.ds(pl.multiple_of(i * depth, depth), depth)
    trows = lambda i: pl.ds(pl.multiple_of(i * LANE, LANE), LANE)

    def kv_copies(d):
        to = lax.rem(s + d, n_sp)
        return (
            remote(keys, k_all.at[rows(s), :], k_sem.at[0, d], k_sem.at[1, d], to, t),
            remote(value, v_all.at[rows(s), :], v_sem.at[0, d], v_sem.at[1, d], to, t),
        )

    def g_copy(d):
        to = lax.rem(s + d, n_sp)
        return remote(g_own, g_all.at[s], g_sem.at[0, d], g_sem.at[1, d], to, t)

    def wo_copy(e):
        to = lax.rem(t + e, n_tp)
        return remote(
            out_w.at[:, lanes(to, features)],
            wo_all.at[pl.ds(pl.multiple_of(t * width, width), width), :],
            wo_sem.at[0, e],
            wo_sem.at[1, e],
            s,
            to,
        )

    def gain_copy(e):
        to = lax.rem(t + e, n_tp)
        return remote(
            gain_own, gain_all.at[:, lanes(t, features)], gain_sem.at[0, e], gain_sem.at[1, e], s, to
        )

    def taps_copy():
        return remote(taps, taps_all.at[core], taps_sem.at[0], taps_sem.at[1], s, partner)

    def tile_ends(tile, slot):
        return (
            (gate_w.at[:, lanes(tile, LANE)], w_up.at[slot, drows(s), pl.ds(0, LANE)]),
            (value_w.at[:, lanes(tile, LANE)], w_up.at[slot, drows(s), pl.ds(LANE, LANE)]),
            (down_w.at[trows(tile), :], w_down.at[trows(slot), lanes(s, cols)]),
        )

    def weight_copies(d):
        to = lax.rem(s + d, n_sp)
        sems = (wg_sem, wv_sem, wd_sem)
        return tuple(
            remote(a, b, sem.at[0, d], sem.at[1, d], to, t)
            for (a, b), sem in zip(tile_ends(to, core), sems)
        )

    def extra_copies(e, source):
        to = e + extras * core
        sems = (xg_sem, xv_sem, xd_sem)
        return tuple(
            remote(a, b, sem.at[0, e], sem.at[1, source], to, t)
            for (a, b), sem in zip(tile_ends(n_sp + e, 2), sems)
        )

    def local_copies():
        pairs = (
            (keys, k_all.at[rows(s), :]),
            (value, v_all.at[rows(s), :]),
            (out_w.at[:, lanes(t, features)],
             wo_all.at[pl.ds(pl.multiple_of(t * width, width), width), :]),
        ) + tile_ends(s, core)
        return tuple(
            pltpu.make_async_copy(a, b, local_sem.at[i]) for i, (a, b) in enumerate(pairs)
        )

    def local_extra(e):
        return tuple(
            pltpu.make_async_copy(a, b, local_x.at[i])
            for i, (a, b) in enumerate(tile_ends(n_sp + e, 2))
        )

    def start_kv(d):
        for copy in kv_copies(d):
            copy.start()

    loop(1, n_sp, start_kv)
    for copy in local_copies():
        copy.start()

    def log_sigmoid(x):
        return jnp.minimum(x, 0.0) - jnp.log1p(jnp.exp(-jnp.abs(x)))

    lf_own[...] = jnp.zeros_like(lf_own)
    lf_own[0:heads, :] = log_sigmoid(gates[1]) + extra_logs[0]
    lf_own[heads : 2 * heads, :] = log_sigmoid(gates[3]) + extra_logs[1]
    lf = lf_own[...]
    row_id = lax.broadcasted_iota(jnp.int32, (tokens, tokens), 0)
    col_id = lax.broadcasted_iota(jnp.int32, (tokens, tokens), 1)
    upto = (row_id >= col_id).astype(F32)
    below = (row_id > col_id).astype(F32)
    row_incl = nt_dot(lf, upto, HIGH)
    row_excl = nt_dot(lf, below, HIGH)
    col_incl = nt_dot(upto, lf, HIGH)
    col_excl = nt_dot(below, lf, HIGH)
    total = jnp.broadcast_to(jnp.sum(lf, axis=1, keepdims=True), lf.shape)
    g_own[0:heads, :] = gates[0] - row_incl[0:heads]
    g_own[heads : 2 * heads, :] = gates[2] + row_excl[heads : 2 * heads]
    g_own[2 * heads : 4 * heads, :] = total[0 : 2 * heads]
    gain_own[...] = jnp.broadcast_to(mixer_gain[...].astype(F32), gain_own.shape)
    g_all[s] = g_own[...]
    gain_all[:, lanes(t, features)] = gain_own[...]
    taps_all[core] = taps[...]
    loop(1, n_sp, lambda d: g_copy(d).start())

    def start_tp(e):
        wo_copy(e).start()
        gain_copy(e).start()

    loop(1, n_tp, start_tp)
    taps_copy().start()

    UP, DOWN = (slice(0, 2), slice(2, 3))

    def start_weights(which):
        def body(d):
            for copy in weight_copies(d)[which]:
                copy.start()

        loop(1, n_sp, body)

    def start_extras(which):
        def body(e):
            @pl.when(e + extras * core != s)
            def _():
                for copy in extra_copies(e, s)[which]:
                    copy.start()

            @pl.when(e + extras * core == s)
            def _():
                for copy in local_extra(e)[which]:
                    copy.start()

        loop(0, extras, body)

    start_weights(UP)
    start_extras(UP)

    loop(1, n_sp, lambda d: g_copy(d).wait_recv())

    def wait_kv(d):
        for copy in kv_copies(d):
            copy.wait_recv()

    for copy in local_copies()[:3]:
        copy.wait()
    g = [g_all[j] for j in range(n_sp)]
    diag_lower = row_id >= col_id
    diag_upper = row_id <= col_id
    logs, peaks = ([], [])
    for h in range(heads):
        acc = jnp.zeros((1, tokens), F32)
        rows_f = [None] * n_sp
        for j in reversed(range(n_sp)):
            acc = acc + jnp.where(j < s, g[j][2 * heads + h : 2 * heads + h + 1], 0.0)
            rows_f[j] = g[j][h : h + 1] + acc
        acc = jnp.zeros((1, tokens), F32)
        logs_h = []
        f_col = col_incl[:, h : h + 1]
        b_col = -col_excl[:, heads + h : heads + h + 1]
        peak = jnp.full((tokens, 1), NEG, F32)
        for j in range(n_sp):
            row_b = g[j][heads + h : heads + h + 1] + acc
            acc = acc + jnp.where(j >= s, g[j][3 * heads + h : 3 * heads + h + 1], 0.0)
            fwd = jnp.where(jnp.logical_or(j < s, jnp.logical_and(j == s, diag_lower)), f_col + rows_f[j], NEG)
            bwd = jnp.where(jnp.logical_or(j > s, jnp.logical_and(j == s, diag_upper)), b_col + row_b, NEG)
            peak = jnp.maximum(peak, jnp.max(jnp.maximum(fwd, bwd), axis=1, keepdims=True))
            logs_h.append((fwd, bwd))
        peaks.append(peak)
        logs.append(
            jnp.concatenate([jnp.exp(f - peak) + jnp.exp(b - peak) for f, b in logs_h], axis=1)
        )
    loop(1, n_sp, wait_kv)
    for h in range(heads):
        lane = slice(h * DH, (h + 1) * DH)
        scores = nt_dot(query[:, lane], k_all[:, lane]) * DH ** (-0.5)
        weighted = (scores * logs[h]).astype(BF16)
        numer = jnp.dot(weighted, v_all[:, lane], preferred_element_type=F32)
        scale = lax.rsqrt(jnp.mean(numer * numer, axis=1, keepdims=True) + EPS)
        gated = (
            numer * scale * head_gain[:, lane].astype(F32)
            * jax.nn.sigmoid(gate_logits[:, lane].astype(F32))
        )
        cell_own[:, lane] = gated.astype(BF16)

    def cell_copy(e):
        to = lax.rem(t + e, n_tp)
        return remote(cell_own, cell_all.at[t], cell_sem.at[0, e], cell_sem.at[1, e], s, to)

    loop(1, n_tp, lambda e: cell_copy(e).start())
    cell_all[t] = cell_own[...]

    def wait_tp(e):
        wo_copy(e).wait_recv()
        gain_copy(e).wait_recv()
        cell_copy(e).wait_recv()

    loop(1, n_tp, wait_tp)
    projected = jnp.zeros((tokens, features), F32)
    for m in range(n_tp):
        piece = jnp.dot(
            cell_all[m], wo_all[m * width : (m + 1) * width, :], preferred_element_type=F32
        )
        projected = projected + piece.astype(BF16).astype(F32)
    stream_own[...] = (resid[...].astype(F32) + projected).astype(BF16)

    place = lax.rem(s, half)

    def x_spot(zl, block_y, m):
        j = 2 * zl + block_y
        return x_all.at[j, :, lanes(m, features)], j * n_tp + m

    def own_shard(j, m):
        return jnp.logical_and(core * half + j == s, m == t)

    def x_copy(d):
        to_z = lax.rem(z + d, half)
        spot, index = x_spot(lax.rem(z, layers), y, t)
        to = (2 * to_z + y, 2 * pair + my_half)
        return remote(stream_own, spot, x_send.at[d], x_recv.at[index], *to)

    def x_pass(zl, block_y, m, send, to):
        spot, index = x_spot(zl, block_y, m)
        return remote(spot, spot, send, x_recv.at[index], *to)

    def stays(d):
        return jnp.logical_and(d == 0, core == my_half)

    def start_x(d):
        @pl.when(jnp.logical_not(stays(d)))
        def _():
            x_copy(d).start()

        @pl.when(stays(d))
        def _():
            x_all[place, :, lanes(t, features)] = stream_own[...]

    loop(0, half, start_x)
    start_weights(DOWN)
    start_extras(DOWN)

    def column(i):
        zl, m = (i // 2, 2 * pair + lax.rem(i, 2))

        @pl.when(jnp.logical_not(own_shard(2 * zl + y, m)))
        def _():
            x_pass(zl, y, m, x_fwd.at[0, i], x_side).wait_recv()

        x_pass(zl, y, m, x_fwd.at[0, i], x_side).start()
        x_pass(zl, y, m, x_fwd.at[1, i], y_side).start()

    loop(0, half, column)

    def relays(zl):
        return (
            x_pass(zl, y, 2 * (1 - pair), x_relay.at[0, zl], y_side),
            x_pass(zl, 1 - y, 2 * pair + 1, x_relay.at[1, zl], x_side),
        )

    def relay(zl):
        for copy in relays(zl):
            copy.wait_recv()
            copy.start()

    loop(0, layers, relay)

    def wait_weights(which):
        def body(d):
            for copy in weight_copies(d)[which]:
                copy.wait_recv()

        loop(1, n_sp, body)

    owner = jnp.logical_and(s >= extras * core, s < extras * (core + 1))
    other_owner = jnp.logical_and(s >= extras * (1 - core), s < extras * (2 - core))

    def forward_copy(slot, down):
        ref = w_down.at[trows(slot), :] if down else w_up.at[slot]
        at = down + (2 if isinstance(slot, int) else 0)
        return remote(ref, ref, fwd_sem.at[0, at], fwd_sem.at[1, at], s, partner)

    def pass_on(down):
        which = DOWN if down else UP
        wait_weights(which)
        for copy in local_copies()[3:][which]:
            copy.wait()
        forward_copy(core, down).start()

        @pl.when(owner)
        def _():
            def wait_extra(source):
                @pl.when(source != s)
                def _():
                    for copy in extra_copies(0, source)[which]:
                        copy.wait_recv()

            loop(0, n_sp, wait_extra)
            for copy in local_extra(0)[which]:
                copy.wait()
            forward_copy(2, down).start()

    def take_other(down):
        forward_copy(1 - core, down).wait_recv()

        @pl.when(other_owner)
        def _():
            forward_copy(2, down).wait_recv()

    @pl.when(s >= 2 * extras)
    def _():
        w_up[2] = jnp.zeros(w_up.shape[1:], BF16)
        w_down[2 * LANE :, :] = jnp.zeros((LANE, w_down.shape[1]), BF16)

    pass_on(0)
    take_other(0)

    def mix_block(i):
        zl, side = (lax.rem(i, layers), i // layers)
        j = 2 * zl + lax.rem(y + side, 2)
        for m in range(n_tp):
            mine = pair == m // 2
            if m % 2 == 0:
                seen = side == 0
            else:
                seen = mine

            @pl.when(jnp.logical_not(seen))
            def _(m=m):
                x_pass(zl, lax.rem(y + side, 2), m, x_relay.at[0, 0], y_side).wait_recv()

        x = x_all[j].astype(F32)
        squares = jnp.sum(x * x, axis=1, keepdims=True)
        normed = (x * lax.rsqrt(squares / model + EPS) * gain_all[0:1, :]).astype(BF16)
        for slot in range(3):
            both = jnp.dot(normed, w_up[slot], preferred_element_type=F32).astype(BF16)
            lane = slice(slot * LANE, (slot + 1) * LANE)
            gate_buf[rows(j), lane] = both[:, :LANE]
            value_buf[rows(j), lane] = both[:, LANE:]

    loop(0, half, mix_block)

    count = half * tokens
    edge = halo.shape[0]

    def halo_copy():
        start = pl.multiple_of((1 - core) * (count - edge), edge)
        return remote(
            gate_buf.at[pl.ds(start, edge), :], halo, halo_sem.at[0], halo_sem.at[1], s, partner
        )

    halo_copy().start()
    pass_on(1)
    taps_copy().wait_recv()
    halo_copy().wait_recv()
    extra_core = jnp.where(s < extras, 0, 1)
    extra_tile = jnp.minimum(n_sp + s - extras * extra_core, tiles - 1)
    slots = ((0, s), (1, s), (extra_core, extra_tile))
    pos = lax.broadcasted_iota(jnp.int32, (count, LANE), 0)
    for slot, (block, tile) in enumerate(slots):
        lane = slice(slot * LANE, (slot + 1) * LANE)
        tap = taps_all[block, :, lanes(tile, LANE)]
        g_mid = gate_buf[:, lane].astype(F32)
        edge_rows = halo[:, lane].astype(F32)
        before = jnp.where(core == 1, edge_rows[edge - 1 : edge], 0.0)
        after = jnp.where(core == 0, edge_rows[0:1], 0.0)
        g_prev = jnp.where(pos == 0, before, pltpu.roll(g_mid, 1, 0))
        g_next = jnp.where(pos == count - 1, after, pltpu.roll(g_mid, count - 1, 0))
        conv = tap[0:1] * g_prev + tap[1:2] * g_mid + tap[2:3] * g_next
        mixed = jax.nn.gelu(conv) * value_buf[:, lane].astype(F32)
        hidden_buf[:, lane] = mixed.astype(BF16)

    take_other(1)

    def product(j, m):
        return jnp.dot(
            hidden_buf[rows(j), :], w_down[:, lanes(m, features)], preferred_element_type=F32
        )

    def first_copies(i):
        return tuple(
            remote(part.at[k, i], part_in.at[k, i], p_sem.at[0, k, i], p_sem.at[1, k, i], *to)
            for k, to in enumerate((x_side, y_side))
        )

    def second_copies(zl):
        return tuple(
            remote(
                part_sum.at[k, zl], sum_in.at[k, zl], q_sem.at[0, k, zl], q_sem.at[1, k, zl], *to
            )
            for k, to in enumerate((y_side, x_side))
        )

    def z_copy(k, zl):
        to = (2 * (core * layers + zl) + y, 2 * pair + k)
        mine = jnp.logical_and(to[0] == s, to[1] == t)
        return mine, remote(z_out.at[k, zl], r_all.at[z], z_send.at[k, zl], r_recv.at[z], *to)

    def first_trip(n):
        zl, late = (lax.rem(n, layers), n // layers)
        by = lax.rem(1 - y + late, 2)
        bx = lax.rem(1 - pair + late, 2)
        i_x, i_y = (2 * zl + by, 2 * zl + bx)
        part[0, i_x] = product(2 * zl + by, 2 * (1 - pair)).astype(BF16)
        first_copies(i_x)[0].start()
        part[1, i_y] = product(2 * zl + 1 - y, 2 * bx + 1).astype(BF16)
        first_copies(i_y)[1].start()

    loop(0, half, first_trip)

    def second_trip(zl):
        i_x, i_y = (2 * zl + 1 - y, 2 * zl + 1 - pair)
        own = product(2 * zl + 1 - y, 2 * pair)
        first_copies(i_x)[0].wait_recv()
        part_sum[0, zl] = (own + part_in[0, i_x].astype(F32)).astype(BF16)
        second_copies(zl)[0].start()
        own = product(2 * zl + y, 2 * (1 - pair) + 1)
        first_copies(i_y)[1].wait_recv()
        part_sum[1, zl] = (own + part_in[1, i_y].astype(F32)).astype(BF16)
        second_copies(zl)[1].start()

    loop(0, layers, second_trip)

    def third_trip(zl):
        for k, i in enumerate((2 * zl + y, 2 * zl + pair)):
            own = product(2 * zl + y, 2 * pair + k)
            first_copies(i)[k].wait_recv()
            own = own + part_in[k, i].astype(F32)
            second_copies(zl)[k].wait_recv()
            result = (own + sum_in[k, zl].astype(F32)).astype(BF16)
            z_out[k, zl] = result
            mine, copy = z_copy(k, zl)

            @pl.when(jnp.logical_not(mine))
            def _():
                copy.start()

            @pl.when(mine)
            def _():
                r_all[z] = result

    loop(0, layers, third_trip)

    out_sum = jnp.zeros((tokens, features), F32)
    for i in range(half):

        @pl.when(jnp.logical_not(jnp.logical_and(core == my_half, z == i)))
        def _(i=i):
            remote(z_out.at[0, 0], r_all.at[i], z_send.at[0, 0], r_recv.at[i], *y_side).wait_recv()

        out_sum = out_sum + r_all[i].astype(F32)
    out[...] = (stream_own[...].astype(F32) + out_sum).astype(BF16)

    def sent_sp(d):
        for copy in kv_copies(d) + (g_copy(d),) + weight_copies(d):
            copy.wait_send()

    loop(1, n_sp, sent_sp)

    def sent_tp(e):
        wo_copy(e).wait_send()
        gain_copy(e).wait_send()
        cell_copy(e).wait_send()

    loop(1, n_tp, sent_tp)
    taps_copy().wait_send()

    def sent_extra(e):
        @pl.when(e + extras * core != s)
        def _():
            for copy in extra_copies(e, s):
                copy.wait_send()

    loop(0, extras, sent_extra)

    def sent_x(d):
        @pl.when(jnp.logical_not(stays(d)))
        def _():
            x_copy(d).wait_send()

        for k, to in enumerate((x_side, y_side)):
            x_pass(d // 2, y, 2 * pair + lax.rem(d, 2), x_fwd.at[k, d], to).wait_send()
        for copy in first_copies(d):
            copy.wait_send()

    loop(0, half, sent_x)

    def sent_layer(zl):
        for copy in relays(zl) + second_copies(zl):
            copy.wait_send()
        for k in range(2):
            mine, copy = z_copy(k, zl)

            @pl.when(jnp.logical_not(mine))
            def _(copy=copy):
                copy.wait_send()

    loop(0, layers, sent_layer)
    for down in range(2):
        forward_copy(core, down).wait_send()

    @pl.when(owner)
    def _():
        for down in range(2):
            forward_copy(2, down).wait_send()

    halo_copy().wait_send()


def fast_layer(n_sp, n_tp, *args):
    (resid, query, keys, value, gate_logits, gates, extra_logs, head_gain, out_w,
     mixer_gain, gate_w, value_w, taps, down_w) = args
    tokens, width = query.shape
    features = resid.shape[1]
    model = features * n_tp
    half = n_sp // 2
    n_pair = n_tp // 2
    hidden = 3 * LANE
    vmem = pl.BlockSpec(memory_space=pltpu.VMEM)
    anywhere = pl.BlockSpec(memory_space=pl.ANY)
    dma = pltpu.SemaphoreType.DMA
    spaces = [vmem, vmem, anywhere, anywhere, vmem, vmem, vmem, vmem, anywhere,
              vmem, anywhere, anywhere, vmem, anywhere]
    scratch = [
        pltpu.VMEM((n_sp * tokens, width), BF16),
        pltpu.VMEM((n_sp * tokens, width), BF16),
        pltpu.VMEM((8, tokens), F32),
        pltpu.VMEM((n_sp, 8, tokens), F32),
        pltpu.VMEM((8, tokens), F32),
        pltpu.VMEM((n_tp * width, features), BF16),
        pltpu.VMEM((2,) + taps.shape, F32),
        pltpu.VMEM((8, features), F32),
        pltpu.VMEM((8, model), F32),
        pltpu.VMEM((3, model, 2 * LANE), BF16),
        pltpu.VMEM((hidden, model), BF16),
        pltpu.VMEM((tokens, width), BF16),
        pltpu.VMEM((n_tp, tokens, width), BF16),
        pltpu.VMEM((tokens, features), BF16),
        pltpu.VMEM((half, tokens, model), BF16),
        pltpu.VMEM((half * tokens, hidden), BF16),
        pltpu.VMEM((half * tokens, hidden), BF16),
        pltpu.VMEM((16, hidden), BF16),
        pltpu.VMEM((half * tokens, hidden), BF16),
        pltpu.VMEM((2, half, tokens, features), BF16),
        pltpu.VMEM((2, half // 2, tokens, features), BF16),
        pltpu.VMEM((2, half, tokens, features), BF16),
        pltpu.VMEM((2, half // 2, tokens, features), BF16),
        pltpu.VMEM((2, half // 2, tokens, features), BF16),
        pltpu.VMEM((half, tokens, features), BF16),
        dma((2, n_sp)),
        dma((2, n_sp)),
        dma((2, n_sp)),
        dma((2, n_tp)),
        dma((2,)),
        dma((2, n_tp)),
        dma((2, n_sp)),
        dma((2, n_sp)),
        dma((2, n_sp)),
        dma((2, n_sp)),
        dma((2, n_sp)),
        dma((2, n_sp)),
        dma((2, 4)),
        dma((2, n_tp)),
        dma((half,)),
        dma((2, half)),
        dma((2, half // 2)),
        dma((half * n_tp,)),
        dma((2,)),
        dma((2, 2, half)),
        dma((2, 2, half // 2)),
        dma((2, half // 2)),
        dma((half,)),
        dma((6,)),
        dma((3,)),
    ]
    return pl.pallas_call(
        functools.partial(layer_kernel, n_sp, n_tp),
        out_shape=jax.ShapeDtypeStruct((tokens, features), BF16),
        in_specs=spaces,
        out_specs=vmem,
        scratch_shapes=scratch,
        compiler_params=pltpu.CompilerParams(has_side_effects=True, vmem_limit_bytes=60 * 2**20),
    )(resid, query, keys, value, gate_logits, gates, extra_logs, head_gain.reshape(1, -1), out_w,
      mixer_gain.reshape(1, -1), gate_w, value_w, taps, down_w)


def choose(n_sp, n_tp, *args):
    tokens, width = args[1].shape
    tiles, rest = divmod(args[10].shape[1], LANE)
    fits = (
        n_sp % 2 == 0
        and n_sp % 4 == 0
        and n_tp == 4
        and rest == 0
        and 0 < tiles - n_sp
        and 2 * (tiles - n_sp) <= n_sp
        and tokens == LANE
        and width == 2 * DH
        and n_sp * tokens <= 1024
    )
    if fits:
        return fast_layer(n_sp, n_tp, *args)
    return per_device(*args)


def solution(mesh):
    return jax.shard_map(
        functools.partial(choose, mesh.shape["sp"], mesh.shape["tp"]),
        mesh=mesh,
        in_specs=(
            P("sp", "tp"),
            P("sp", "tp"),
            P("sp", "tp"),
            P("sp", "tp"),
            P("sp", "tp"),
            P(None, "tp", "sp"),
            P(None, "tp", "sp"),
            P("tp"),
            P("tp", None),
            P("tp"),
            P("sp", "tp"),
            P("sp", "tp"),
            P(None, "tp"),
            P("tp", "sp"),
        ),
        out_specs=P("sp", "tp"),
        check_vma=False,
    )
```

```python
import functools

import jax
import jax.numpy as jnp
from jax import lax
from jax.experimental import pallas as pl
from jax.experimental.pallas import tpu as pltpu
from jax.sharding import PartitionSpec as P

D = 2048
DH = 128
BLOCK = 64


NEG = -1e30
EPS = 1e-06
HIGH = lax.Precision.HIGHEST


def entering(array, axis, combine, identity, reverse):
    size, here = (lax.axis_size(axis), lax.axis_index(axis))
    everything = jax.tree.map(lambda part: lax.all_gather(part, axis), array)
    start = jax.tree.map(
        lambda part, zero: jnp.broadcast_to(jnp.asarray(zero, part.dtype), part.shape),
        array,
        identity,
    )

    def lap(k, before):
        at = size - 1 - k if reverse else k
        reached = at > here if reverse else at < here
        new = combine(before, jax.tree.map(lambda part: part[at], everything))
        return jax.tree.map(lambda a, b: jnp.where(reached, a, b), new, before)

    return lax.fori_loop(0, size, lap, start)


def extended(array, sides, width):
    for axis, dim in sides:
        size, length = (lax.axis_size(axis), array.shape[dim])
        up = [(i, (i + 1) % size) for i in range(size - 1)]
        down = [(j, i) for i, j in up]
        last = lax.slice_in_dim(array, length - width, length, axis=dim)
        first = lax.slice_in_dim(array, 0, width, axis=dim)
        before = lax.ppermute(last, axis, up)
        after = lax.ppermute(first, axis, down)
        array = jnp.concatenate([before, array, after], axis=dim)
    return array


def heads_blocks(source, head_count):
    length = source.shape[0]
    shaped = source.astype(jnp.float32).reshape(length // BLOCK, BLOCK, head_count, DH)
    return shaped.transpose(2, 0, 1, 3)


def merge_states(earlier, later):
    c_early, m_early, b_early = earlier
    c_late, m_late, b_late = later
    m_new = jnp.maximum(b_late + m_early, m_late)
    c_new = (
        jnp.exp(b_late + m_early - m_new)[..., None, None] * c_early
        + jnp.exp(m_late - m_new)[..., None, None] * c_late
    )
    return (c_new, m_new, b_early + b_late)


def carry_step(carry, inputs):
    return (merge_states(carry, inputs), carry)


def block_terms(key_rows, values, log_in, log_forget):
    cumulative = jnp.cumsum(log_forget, axis=-1)
    block_end = cumulative[..., -1]
    weight_log = block_end[..., None] - cumulative + log_in
    m_local = jnp.max(weight_log, axis=-1)
    weights = jnp.exp(weight_log - m_local[..., None])
    c_local = jnp.einsum("hnsd,hnse->hnde", weights[..., None] * key_rows, values, precision=HIGH)
    return (cumulative, block_end, m_local, c_local)


def block_output(queries, key_rows, values, log_in, cumulative, c_start, m_start):
    a_log = cumulative + m_start[..., None]
    d_log = cumulative[..., :, None] - cumulative[..., None, :] + log_in[..., None, :]
    block_len = cumulative.shape[-1]
    lower_mask = jnp.arange(block_len)[:, None] >= jnp.arange(block_len)[None, :]
    d_log = jnp.where(lower_mask, d_log, -jnp.inf)
    m_row = jnp.maximum(a_log, jnp.max(d_log, axis=-1))
    decays = jnp.exp(d_log - m_row[..., None])
    carried = jnp.exp(a_log - m_row)
    scores = jnp.einsum("hntd,hnsd->hnts", queries, key_rows, precision=HIGH) * decays
    numerator = jnp.einsum("hnts,hnse->hnte", scores, values, precision=HIGH) + carried[
        ..., None
    ] * jnp.einsum("hntd,hnde->hnte", queries, c_start, precision=HIGH)
    return (numerator, m_row)


def single_direction(query, memory_keys, value, log_in, log_forget, reverse):
    head_count = query.shape[1] // DH
    nblocks = query.shape[0] // BLOCK
    queries = heads_blocks(query, head_count)
    key_rows = heads_blocks(memory_keys, head_count) * DH ** (-0.5)
    values = heads_blocks(value, head_count)
    log_in = log_in.reshape(head_count, nblocks, BLOCK)
    log_forget = log_forget.reshape(head_count, nblocks, BLOCK)
    cumulative, block_end, m_local, c_local = block_terms(key_rows, values, log_in, log_forget)
    identity = (
        jnp.zeros((head_count, DH, DH), jnp.float32),
        jnp.full((head_count,), NEG, jnp.float32),
        jnp.zeros((head_count,), jnp.float32),
    )
    totals, prefix = lax.scan(
        carry_step, identity, (jnp.moveaxis(c_local, 1, 0), m_local.T, block_end.T)
    )
    if reverse:
        incoming = entering(totals, "sp", merge_states, identity, True)
    else:
        incoming = entering(totals, "sp", merge_states, identity, False)
    starts = merge_states(tuple((member[None] for member in incoming)), prefix)
    c_start = jnp.moveaxis(starts[0], 0, 1)
    m_start = starts[1].T
    numerator, m_row = block_output(queries, key_rows, values, log_in, cumulative, c_start, m_start)
    return (numerator.reshape(head_count, -1, DH), m_row.reshape(head_count, -1))


def per_device(
    resid,
    query,
    memory_keys,
    value,
    output_gate_logits,
    gate_preactivation,
    extra_forget_logs,
    head_norm_gain,
    output_weight,
    mixer_norm_gain,
    gate_up_weight,
    value_up_weight,
    convolution_weight,
    down_weight,
):
    tokens = query.shape[0]
    forward_numerator, forward_peak = single_direction(
        query,
        memory_keys,
        value,
        gate_preactivation[0],
        jax.nn.log_sigmoid(gate_preactivation[1]) + extra_forget_logs[0],
        False,
    )
    backward_numerator, backward_peak = single_direction(
        jnp.flip(query, 0),
        jnp.flip(memory_keys, 0),
        jnp.flip(value, 0),
        jnp.flip(gate_preactivation[2], -1),
        jnp.flip(jax.nn.log_sigmoid(gate_preactivation[3]) + extra_forget_logs[1], -1),
        True,
    )
    backward_numerator = jnp.flip(backward_numerator, 1)
    backward_peak = jnp.flip(backward_peak, 1)
    both_max = jnp.maximum(forward_peak, backward_peak)
    numerator = (
        jnp.exp(forward_peak - both_max)[..., None] * forward_numerator
        + jnp.exp(backward_peak - both_max)[..., None] * backward_numerator
    )
    normal_cell = numerator * lax.rsqrt(
        jnp.mean(numerator * numerator, axis=-1, keepdims=True) + EPS
    )
    cell = normal_cell.transpose(1, 0, 2).reshape(tokens, -1)
    cell = (
        cell
        * head_norm_gain.astype(jnp.float32)
        * jax.nn.sigmoid(output_gate_logits.astype(jnp.float32))
    ).astype(jnp.bfloat16)
    partial_proj = jnp.dot(cell, output_weight, preferred_element_type=jnp.float32)
    stream = (
        resid.astype(jnp.float32)
        + lax.psum_scatter(
            partial_proj.astype(jnp.bfloat16), "tp", scatter_dimension=1, tiled=True
        ).astype(jnp.float32)
    ).astype(jnp.bfloat16)
    stream_f = stream.astype(jnp.float32)
    squares = lax.psum(jnp.sum(stream_f * stream_f, axis=1), "tp")
    normed_own = (
        stream_f * lax.rsqrt(squares / D + EPS)[:, None] * mixer_norm_gain.astype(jnp.float32)
    ).astype(jnp.bfloat16)
    normed = lax.all_gather(normed_own, "tp", axis=1, tiled=True)
    gate_sum = jnp.dot(
        normed,
        lax.all_gather(gate_up_weight, "sp", axis=0, tiled=True),
        preferred_element_type=jnp.float32,
    )
    value_sum = jnp.dot(
        normed,
        lax.all_gather(value_up_weight, "sp", axis=0, tiled=True),
        preferred_element_type=jnp.float32,
    )
    gate_mix = gate_sum.astype(jnp.bfloat16)
    value_mix = value_sum.astype(jnp.bfloat16)
    padded = extended(gate_mix, (("sp", 0),), 1)
    padded_f = padded.astype(jnp.float32)
    convolved = (
        convolution_weight[0] * padded_f[:-2]
        + convolution_weight[1] * padded_f[1:-1]
        + convolution_weight[2] * padded_f[2:]
    )
    hidden = (jax.nn.gelu(convolved) * value_mix.astype(jnp.float32)).astype(jnp.bfloat16)
    down_term = jnp.dot(
        hidden,
        lax.all_gather(down_weight, "sp", axis=1, tiled=True),
        preferred_element_type=jnp.float32,
    )
    mixer_out = lax.psum_scatter(
        down_term.astype(jnp.bfloat16), "tp", scatter_dimension=1, tiled=True
    ).astype(jnp.float32)
    return (stream.astype(jnp.float32) + mixer_out).astype(jnp.bfloat16)


LANE = 128
MESH = pl.DeviceIdType.MESH
F32 = jnp.float32
BF16 = jnp.bfloat16


def remote(src, dst, send, recv, sp, tp):
    return pltpu.make_async_remote_copy(
        src_ref=src,
        dst_ref=dst,
        send_sem=send,
        recv_sem=recv,
        device_id=(sp, tp),
        device_id_type=MESH,
    )


def nt_dot(a, b, precision=None):
    return lax.dot_general(
        a, b, (((1,), (1,)), ((), ())), precision=precision, preferred_element_type=F32
    )


def layer_kernel(
    n_sp,
    n_tp,
    resid,
    query,
    keys,
    value,
    gate_logits,
    gates,
    extra_logs,
    head_gain,
    out_w,
    mixer_gain,
    gate_w,
    value_w,
    taps,
    down_w,
    out,
    k_all,
    v_all,
    g_own,
    g_all,
    lf_own,
    wo_all,
    taps_all,
    gain_own,
    gain_all,
    w_up,
    w_down,
    cell_own,
    cell_all,
    stream_own,
    x_all,
    gate_buf,
    value_buf,
    halo,
    hidden_buf,
    part,
    part_sum,
    part_in,
    sum_in,
    z_out,
    r_all,
    k_sem,
    v_sem,
    g_sem,
    wo_sem,
    taps_sem,
    gain_sem,
    wg_sem,
    wv_sem,
    wd_sem,
    xg_sem,
    xv_sem,
    xd_sem,
    fwd_sem,
    cell_sem,
    x_send,
    x_fwd,
    x_relay,
    x_recv,
    halo_sem,
    p_sem,
    q_sem,
    z_send,
    r_recv,
    local_sem,
    local_x,
):
    s, t = (lax.axis_index("sp"), lax.axis_index("tp"))
    core = lax.rem(t, 2)
    pair = t // 2
    partner = t + 1 - 2 * core
    n_pair = n_tp // 2
    tokens = query.shape[0]
    width = query.shape[1]
    features = resid.shape[1]
    depth = gate_w.shape[0]
    cols = down_w.shape[1]
    heads = width // DH
    tiles = gate_w.shape[1] // LANE
    extras = tiles - n_sp
    half = n_sp // 2
    my_half = s // half
    model = features * n_tp
    z, y = (s // 2, lax.rem(s, 2))
    layers = half // 2
    x_side = (s, 2 * (1 - pair) + core)
    y_side = (2 * z + 1 - y, t)

    def loop(low, high, body):
        def step(i, carry):
            body(i)
            return carry

        lax.fori_loop(low, high, step, 0)

    rows = lambda i: pl.ds(pl.multiple_of(i * tokens, tokens), tokens)
    lanes = lambda i, size: pl.ds(pl.multiple_of(i * size, LANE), size)
    drows = lambda i: pl.ds(pl.multiple_of(i * depth, depth), depth)
    trows = lambda i: pl.ds(pl.multiple_of(i * LANE, LANE), LANE)

    def kv_copies(d):
        to = lax.rem(s + d, n_sp)
        return (
            remote(keys, k_all.at[rows(s), :], k_sem.at[0, d], k_sem.at[1, d], to, t),
            remote(value, v_all.at[rows(s), :], v_sem.at[0, d], v_sem.at[1, d], to, t),
        )

    def g_copy(d):
        to = lax.rem(s + d, n_sp)
        return remote(g_own, g_all.at[s], g_sem.at[0, d], g_sem.at[1, d], to, t)

    def wo_copy(e):
        to = lax.rem(t + e, n_tp)
        return remote(
            out_w.at[:, lanes(to, features)],
            wo_all.at[pl.ds(pl.multiple_of(t * width, width), width), :],
            wo_sem.at[0, e],
            wo_sem.at[1, e],
            s,
            to,
        )

    def gain_copy(e):
        to = lax.rem(t + e, n_tp)
        return remote(
            gain_own, gain_all.at[:, lanes(t, features)], gain_sem.at[0, e], gain_sem.at[1, e], s, to
        )

    def taps_copy():
        return remote(taps, taps_all.at[core], taps_sem.at[0], taps_sem.at[1], s, partner)

    def tile_ends(tile, slot):
        return (
            (gate_w.at[:, lanes(tile, LANE)], w_up.at[slot, drows(s), pl.ds(0, LANE)]),
            (value_w.at[:, lanes(tile, LANE)], w_up.at[slot, drows(s), pl.ds(LANE, LANE)]),
            (down_w.at[trows(tile), :], w_down.at[trows(slot), lanes(s, cols)]),
        )

    def weight_copies(d):
        to = lax.rem(s + d, n_sp)
        sems = (wg_sem, wv_sem, wd_sem)
        return tuple(
            remote(a, b, sem.at[0, d], sem.at[1, d], to, t)
            for (a, b), sem in zip(tile_ends(to, core), sems)
        )

    def extra_copies(e, source):
        to = e + extras * core
        sems = (xg_sem, xv_sem, xd_sem)
        return tuple(
            remote(a, b, sem.at[0, e], sem.at[1, source], to, t)
            for (a, b), sem in zip(tile_ends(n_sp + e, 2), sems)
        )

    def local_copies():
        pairs = (
            (keys, k_all.at[rows(s), :]),
            (value, v_all.at[rows(s), :]),
            (out_w.at[:, lanes(t, features)],
             wo_all.at[pl.ds(pl.multiple_of(t * width, width), width), :]),
        ) + tile_ends(s, core)
        return tuple(
            pltpu.make_async_copy(a, b, local_sem.at[i]) for i, (a, b) in enumerate(pairs)
        )

    def local_extra(e):
        return tuple(
            pltpu.make_async_copy(a, b, local_x.at[i])
            for i, (a, b) in enumerate(tile_ends(n_sp + e, 2))
        )

    barrier = pltpu.get_barrier_semaphore()

    def greet(to_s, to_t):
        pl.semaphore_signal(barrier, inc=1, device_id=(to_s, to_t), device_id_type=MESH)

    loop(1, n_sp, lambda d: greet(lax.rem(s + d, n_sp), t))
    loop(1, n_tp, lambda e: greet(s, lax.rem(t + e, n_tp)))
    loop(1, half, lambda d: greet(2 * lax.rem(z + d, half) + y, partner))
    pl.semaphore_wait(barrier, n_sp + n_tp + half - 3)

    def start_kv(d):
        for copy in kv_copies(d):
            copy.start()

    loop(1, n_sp, start_kv)
    for copy in local_copies():
        copy.start()

    def log_sigmoid(x):
        return jnp.minimum(x, 0.0) - jnp.log1p(jnp.exp(-jnp.abs(x)))

    lf_own[...] = jnp.zeros_like(lf_own)
    lf_own[0:heads, :] = log_sigmoid(gates[1]) + extra_logs[0]
    lf_own[heads : 2 * heads, :] = log_sigmoid(gates[3]) + extra_logs[1]
    lf = lf_own[...]
    row_id = lax.broadcasted_iota(jnp.int32, (tokens, tokens), 0)
    col_id = lax.broadcasted_iota(jnp.int32, (tokens, tokens), 1)
    upto = (row_id >= col_id).astype(F32)
    below = (row_id > col_id).astype(F32)
    row_incl = nt_dot(lf, upto, HIGH)
    row_excl = nt_dot(lf, below, HIGH)
    col_incl = nt_dot(upto, lf, HIGH)
    col_excl = nt_dot(below, lf, HIGH)
    total = jnp.broadcast_to(jnp.sum(lf, axis=1, keepdims=True), lf.shape)
    g_own[0:heads, :] = gates[0] - row_incl[0:heads]
    g_own[heads : 2 * heads, :] = gates[2] + row_excl[heads : 2 * heads]
    g_own[2 * heads : 4 * heads, :] = total[0 : 2 * heads]
    gain_own[...] = jnp.broadcast_to(mixer_gain[...].astype(F32), gain_own.shape)
    g_all[s] = g_own[...]
    gain_all[:, lanes(t, features)] = gain_own[...]
    taps_all[core] = taps[...]
    loop(1, n_sp, lambda d: g_copy(d).start())

    def start_tp(e):
        wo_copy(e).start()
        gain_copy(e).start()

    loop(1, n_tp, start_tp)
    taps_copy().start()

    UP, DOWN = (slice(0, 2), slice(2, 3))

    def start_weights(which):
        def body(d):
            for copy in weight_copies(d)[which]:
                copy.start()

        loop(1, n_sp, body)

    def start_extras(which):
        def body(e):
            @pl.when(e + extras * core != s)
            def _():
                for copy in extra_copies(e, s)[which]:
                    copy.start()

            @pl.when(e + extras * core == s)
            def _():
                for copy in local_extra(e)[which]:
                    copy.start()

        loop(0, extras, body)

    start_weights(UP)
    start_extras(UP)

    loop(1, n_sp, lambda d: g_copy(d).wait_recv())

    def wait_kv(d):
        for copy in kv_copies(d):
            copy.wait_recv()

    for copy in local_copies()[:3]:
        copy.wait()
    g = [g_all[j] for j in range(n_sp)]
    diag_lower = row_id >= col_id
    diag_upper = row_id <= col_id
    logs, peaks = ([], [])
    for h in range(heads):
        acc = jnp.zeros((1, tokens), F32)
        rows_f = [None] * n_sp
        for j in reversed(range(n_sp)):
            acc = acc + jnp.where(j < s, g[j][2 * heads + h : 2 * heads + h + 1], 0.0)
            rows_f[j] = g[j][h : h + 1] + acc
        acc = jnp.zeros((1, tokens), F32)
        logs_h = []
        f_col = col_incl[:, h : h + 1]
        b_col = -col_excl[:, heads + h : heads + h + 1]
        peak = jnp.full((tokens, 1), NEG, F32)
        for j in range(n_sp):
            row_b = g[j][heads + h : heads + h + 1] + acc
            acc = acc + jnp.where(j >= s, g[j][3 * heads + h : 3 * heads + h + 1], 0.0)
            fwd = jnp.where(jnp.logical_or(j < s, jnp.logical_and(j == s, diag_lower)), f_col + rows_f[j], NEG)
            bwd = jnp.where(jnp.logical_or(j > s, jnp.logical_and(j == s, diag_upper)), b_col + row_b, NEG)
            peak = jnp.maximum(peak, jnp.max(jnp.maximum(fwd, bwd), axis=1, keepdims=True))
            logs_h.append((fwd, bwd))
        peaks.append(peak)
        logs.append(
            jnp.concatenate([jnp.exp(f - peak) + jnp.exp(b - peak) for f, b in logs_h], axis=1)
        )
    loop(1, n_sp, wait_kv)
    for h in range(heads):
        lane = slice(h * DH, (h + 1) * DH)
        scores = nt_dot(query[:, lane], k_all[:, lane]) * DH ** (-0.5)
        weighted = (scores * logs[h]).astype(BF16)
        numer = jnp.dot(weighted, v_all[:, lane], preferred_element_type=F32)
        scale = lax.rsqrt(jnp.mean(numer * numer, axis=1, keepdims=True) + EPS)
        gated = (
            numer * scale * head_gain[:, lane].astype(F32)
            * jax.nn.sigmoid(gate_logits[:, lane].astype(F32))
        )
        cell_own[:, lane] = gated.astype(BF16)

    def cell_copy(e):
        to = lax.rem(t + e, n_tp)
        return remote(cell_own, cell_all.at[t], cell_sem.at[0, e], cell_sem.at[1, e], s, to)

    loop(1, n_tp, lambda e: cell_copy(e).start())
    cell_all[t] = cell_own[...]

    def wait_tp(e):
        wo_copy(e).wait_recv()
        gain_copy(e).wait_recv()
        cell_copy(e).wait_recv()

    loop(1, n_tp, wait_tp)
    projected = jnp.zeros((tokens, features), F32)
    for m in range(n_tp):
        piece = jnp.dot(
            cell_all[m], wo_all[m * width : (m + 1) * width, :], preferred_element_type=F32
        )
        projected = projected + piece.astype(BF16).astype(F32)
    stream_own[...] = (resid[...].astype(F32) + projected).astype(BF16)

    place = lax.rem(s, half)

    def x_spot(zl, block_y, m):
        j = 2 * zl + block_y
        return x_all.at[j, :, lanes(m, features)], j * n_tp + m

    def own_shard(j, m):
        return jnp.logical_and(core * half + j == s, m == t)

    def x_copy(d):
        to_z = lax.rem(z + d, half)
        spot, index = x_spot(lax.rem(z, layers), y, t)
        to = (2 * to_z + y, 2 * pair + my_half)
        return remote(stream_own, spot, x_send.at[d], x_recv.at[index], *to)

    def x_pass(zl, block_y, m, send, to):
        spot, index = x_spot(zl, block_y, m)
        return remote(spot, spot, send, x_recv.at[index], *to)

    def stays(d):
        return jnp.logical_and(d == 0, core == my_half)

    def start_x(d):
        @pl.when(jnp.logical_not(stays(d)))
        def _():
            x_copy(d).start()

        @pl.when(stays(d))
        def _():
            x_all[place, :, lanes(t, features)] = stream_own[...]

    loop(0, half, start_x)
    start_weights(DOWN)
    start_extras(DOWN)

    def column(i):
        zl, m = (i // 2, 2 * pair + lax.rem(i, 2))

        @pl.when(jnp.logical_not(own_shard(2 * zl + y, m)))
        def _():
            x_pass(zl, y, m, x_fwd.at[0, i], x_side).wait_recv()

        x_pass(zl, y, m, x_fwd.at[0, i], x_side).start()
        x_pass(zl, y, m, x_fwd.at[1, i], y_side).start()

    loop(0, half, column)

    def relays(zl):
        return (
            x_pass(zl, y, 2 * (1 - pair), x_relay.at[0, zl], y_side),
            x_pass(zl, 1 - y, 2 * pair + 1, x_relay.at[1, zl], x_side),
        )

    def relay(zl):
        for copy in relays(zl):
            copy.wait_recv()
            copy.start()

    loop(0, layers, relay)

    def wait_weights(which):
        def body(d):
            for copy in weight_copies(d)[which]:
                copy.wait_recv()

        loop(1, n_sp, body)

    owner = jnp.logical_and(s >= extras * core, s < extras * (core + 1))
    other_owner = jnp.logical_and(s >= extras * (1 - core), s < extras * (2 - core))

    def forward_copy(slot, down):
        ref = w_down.at[trows(slot), :] if down else w_up.at[slot]
        at = down + (2 if isinstance(slot, int) else 0)
        return remote(ref, ref, fwd_sem.at[0, at], fwd_sem.at[1, at], s, partner)

    def pass_on(down):
        which = DOWN if down else UP
        wait_weights(which)
        for copy in local_copies()[3:][which]:
            copy.wait()
        forward_copy(core, down).start()

        @pl.when(owner)
        def _():
            def wait_extra(source):
                @pl.when(source != s)
                def _():
                    for copy in extra_copies(0, source)[which]:
                        copy.wait_recv()

            loop(0, n_sp, wait_extra)
            for copy in local_extra(0)[which]:
                copy.wait()
            forward_copy(2, down).start()

    def take_other(down):
        forward_copy(1 - core, down).wait_recv()

        @pl.when(other_owner)
        def _():
            forward_copy(2, down).wait_recv()

    @pl.when(s >= 2 * extras)
    def _():
        w_up[2] = jnp.zeros(w_up.shape[1:], BF16)
        w_down[2 * LANE :, :] = jnp.zeros((LANE, w_down.shape[1]), BF16)

    pass_on(0)
    take_other(0)

    def mix_block(i):
        zl, side = (lax.rem(i, layers), i // layers)
        j = 2 * zl + lax.rem(y + side, 2)
        for m in range(n_tp):
            mine = pair == m // 2
            if m % 2 == 0:
                seen = side == 0
            else:
                seen = mine

            @pl.when(jnp.logical_not(seen))
            def _(m=m):
                x_pass(zl, lax.rem(y + side, 2), m, x_relay.at[0, 0], y_side).wait_recv()

        x = x_all[j].astype(F32)
        squares = jnp.sum(x * x, axis=1, keepdims=True)
        normed = (x * lax.rsqrt(squares / model + EPS) * gain_all[0:1, :]).astype(BF16)
        for slot in range(3):
            both = jnp.dot(normed, w_up[slot], preferred_element_type=F32).astype(BF16)
            lane = slice(slot * LANE, (slot + 1) * LANE)
            gate_buf[rows(j), lane] = both[:, :LANE]
            value_buf[rows(j), lane] = both[:, LANE:]

    loop(0, half, mix_block)

    count = half * tokens
    edge = halo.shape[0]

    def halo_copy():
        start = pl.multiple_of((1 - core) * (count - edge), edge)
        return remote(
            gate_buf.at[pl.ds(start, edge), :], halo, halo_sem.at[0], halo_sem.at[1], s, partner
        )

    halo_copy().start()
    pass_on(1)
    taps_copy().wait_recv()
    halo_copy().wait_recv()
    extra_core = jnp.where(s < extras, 0, 1)
    extra_tile = jnp.minimum(n_sp + s - extras * extra_core, tiles - 1)
    slots = ((0, s), (1, s), (extra_core, extra_tile))
    pos = lax.broadcasted_iota(jnp.int32, (count, LANE), 0)
    for slot, (block, tile) in enumerate(slots):
        lane = slice(slot * LANE, (slot + 1) * LANE)
        tap = taps_all[block, :, lanes(tile, LANE)]
        g_mid = gate_buf[:, lane].astype(F32)
        edge_rows = halo[:, lane].astype(F32)
        before = jnp.where(core == 1, edge_rows[edge - 1 : edge], 0.0)
        after = jnp.where(core == 0, edge_rows[0:1], 0.0)
        g_prev = jnp.where(pos == 0, before, pltpu.roll(g_mid, 1, 0))
        g_next = jnp.where(pos == count - 1, after, pltpu.roll(g_mid, count - 1, 0))
        conv = tap[0:1] * g_prev + tap[1:2] * g_mid + tap[2:3] * g_next
        mixed = jax.nn.gelu(conv) * value_buf[:, lane].astype(F32)
        hidden_buf[:, lane] = mixed.astype(BF16)

    take_other(1)

    def product(j, m):
        return jnp.dot(
            hidden_buf[rows(j), :], w_down[:, lanes(m, features)], preferred_element_type=F32
        )

    def first_copies(i):
        return tuple(
            remote(part.at[k, i], part_in.at[k, i], p_sem.at[0, k, i], p_sem.at[1, k, i], *to)
            for k, to in enumerate((x_side, y_side))
        )

    def second_copies(zl):
        return tuple(
            remote(
                part_sum.at[k, zl], sum_in.at[k, zl], q_sem.at[0, k, zl], q_sem.at[1, k, zl], *to
            )
            for k, to in enumerate((y_side, x_side))
        )

    def z_copy(k, zl):
        to = (2 * (core * layers + zl) + y, 2 * pair + k)
        mine = jnp.logical_and(to[0] == s, to[1] == t)
        return mine, remote(z_out.at[k, zl], r_all.at[z], z_send.at[k, zl], r_recv.at[z], *to)

    def first_trip(n):
        zl, late = (lax.rem(n, layers), n // layers)
        by = lax.rem(1 - y + late, 2)
        bx = lax.rem(1 - pair + late, 2)
        i_x, i_y = (2 * zl + by, 2 * zl + bx)
        part[0, i_x] = product(2 * zl + by, 2 * (1 - pair)).astype(BF16)
        first_copies(i_x)[0].start()
        part[1, i_y] = product(2 * zl + 1 - y, 2 * bx + 1).astype(BF16)
        first_copies(i_y)[1].start()

    loop(0, half, first_trip)

    def second_trip(zl):
        i_x, i_y = (2 * zl + 1 - y, 2 * zl + 1 - pair)
        own = product(2 * zl + 1 - y, 2 * pair)
        first_copies(i_x)[0].wait_recv()
        part_sum[0, zl] = (own + part_in[0, i_x].astype(F32)).astype(BF16)
        second_copies(zl)[0].start()
        own = product(2 * zl + y, 2 * (1 - pair) + 1)
        first_copies(i_y)[1].wait_recv()
        part_sum[1, zl] = (own + part_in[1, i_y].astype(F32)).astype(BF16)
        second_copies(zl)[1].start()

    loop(0, layers, second_trip)

    def third_trip(zl):
        for k, i in enumerate((2 * zl + y, 2 * zl + pair)):
            own = product(2 * zl + y, 2 * pair + k)
            first_copies(i)[k].wait_recv()
            own = own + part_in[k, i].astype(F32)
            second_copies(zl)[k].wait_recv()
            result = (own + sum_in[k, zl].astype(F32)).astype(BF16)
            z_out[k, zl] = result
            mine, copy = z_copy(k, zl)

            @pl.when(jnp.logical_not(mine))
            def _():
                copy.start()

            @pl.when(mine)
            def _():
                r_all[z] = result

    loop(0, layers, third_trip)

    out_sum = jnp.zeros((tokens, features), F32)
    for i in range(half):

        @pl.when(jnp.logical_not(jnp.logical_and(core == my_half, z == i)))
        def _(i=i):
            remote(z_out.at[0, 0], r_all.at[i], z_send.at[0, 0], r_recv.at[i], *y_side).wait_recv()

        out_sum = out_sum + r_all[i].astype(F32)
    out[...] = (stream_own[...].astype(F32) + out_sum).astype(BF16)

    def sent_sp(d):
        for copy in kv_copies(d) + (g_copy(d),) + weight_copies(d):
            copy.wait_send()

    loop(1, n_sp, sent_sp)

    def sent_tp(e):
        wo_copy(e).wait_send()
        gain_copy(e).wait_send()
        cell_copy(e).wait_send()

    loop(1, n_tp, sent_tp)
    taps_copy().wait_send()

    def sent_extra(e):
        @pl.when(e + extras * core != s)
        def _():
            for copy in extra_copies(e, s):
                copy.wait_send()

    loop(0, extras, sent_extra)

    def sent_x(d):
        @pl.when(jnp.logical_not(stays(d)))
        def _():
            x_copy(d).wait_send()

        for k, to in enumerate((x_side, y_side)):
            x_pass(d // 2, y, 2 * pair + lax.rem(d, 2), x_fwd.at[k, d], to).wait_send()
        for copy in first_copies(d):
            copy.wait_send()

    loop(0, half, sent_x)

    def sent_layer(zl):
        for copy in relays(zl) + second_copies(zl):
            copy.wait_send()
        for k in range(2):
            mine, copy = z_copy(k, zl)

            @pl.when(jnp.logical_not(mine))
            def _(copy=copy):
                copy.wait_send()

    loop(0, layers, sent_layer)
    for down in range(2):
        forward_copy(core, down).wait_send()

    @pl.when(owner)
    def _():
        for down in range(2):
            forward_copy(2, down).wait_send()

    halo_copy().wait_send()


def fast_layer(n_sp, n_tp, *args):
    (resid, query, keys, value, gate_logits, gates, extra_logs, head_gain, out_w,
     mixer_gain, gate_w, value_w, taps, down_w) = args
    tokens, width = query.shape
    features = resid.shape[1]
    model = features * n_tp
    half = n_sp // 2
    n_pair = n_tp // 2
    hidden = 3 * LANE
    vmem = pl.BlockSpec(memory_space=pltpu.VMEM)
    anywhere = pl.BlockSpec(memory_space=pl.ANY)
    dma = pltpu.SemaphoreType.DMA
    spaces = [vmem, vmem, anywhere, anywhere, vmem, vmem, vmem, vmem, anywhere,
              vmem, anywhere, anywhere, vmem, anywhere]
    scratch = [
        pltpu.VMEM((n_sp * tokens, width), BF16),
        pltpu.VMEM((n_sp * tokens, width), BF16),
        pltpu.VMEM((8, tokens), F32),
        pltpu.VMEM((n_sp, 8, tokens), F32),
        pltpu.VMEM((8, tokens), F32),
        pltpu.VMEM((n_tp * width, features), BF16),
        pltpu.VMEM((2,) + taps.shape, F32),
        pltpu.VMEM((8, features), F32),
        pltpu.VMEM((8, model), F32),
        pltpu.VMEM((3, model, 2 * LANE), BF16),
        pltpu.VMEM((hidden, model), BF16),
        pltpu.VMEM((tokens, width), BF16),
        pltpu.VMEM((n_tp, tokens, width), BF16),
        pltpu.VMEM((tokens, features), BF16),
        pltpu.VMEM((half, tokens, model), BF16),
        pltpu.VMEM((half * tokens, hidden), BF16),
        pltpu.VMEM((half * tokens, hidden), BF16),
        pltpu.VMEM((16, hidden), BF16),
        pltpu.VMEM((half * tokens, hidden), BF16),
        pltpu.VMEM((2, half, tokens, features), BF16),
        pltpu.VMEM((2, half // 2, tokens, features), BF16),
        pltpu.VMEM((2, half, tokens, features), BF16),
        pltpu.VMEM((2, half // 2, tokens, features), BF16),
        pltpu.VMEM((2, half // 2, tokens, features), BF16),
        pltpu.VMEM((half, tokens, features), BF16),
        dma((2, n_sp)),
        dma((2, n_sp)),
        dma((2, n_sp)),
        dma((2, n_tp)),
        dma((2,)),
        dma((2, n_tp)),
        dma((2, n_sp)),
        dma((2, n_sp)),
        dma((2, n_sp)),
        dma((2, n_sp)),
        dma((2, n_sp)),
        dma((2, n_sp)),
        dma((2, 4)),
        dma((2, n_tp)),
        dma((half,)),
        dma((2, half)),
        dma((2, half // 2)),
        dma((half * n_tp,)),
        dma((2,)),
        dma((2, 2, half)),
        dma((2, 2, half // 2)),
        dma((2, half // 2)),
        dma((half,)),
        dma((6,)),
        dma((3,)),
    ]
    return pl.pallas_call(
        functools.partial(layer_kernel, n_sp, n_tp),
        out_shape=jax.ShapeDtypeStruct((tokens, features), BF16),
        in_specs=spaces,
        out_specs=vmem,
        scratch_shapes=scratch,
        compiler_params=pltpu.CompilerParams(has_side_effects=True, collective_id=0, vmem_limit_bytes=60 * 2**20),
    )(resid, query, keys, value, gate_logits, gates, extra_logs, head_gain.reshape(1, -1), out_w,
      mixer_gain.reshape(1, -1), gate_w, value_w, taps, down_w)


def choose(n_sp, n_tp, *args):
    tokens, width = args[1].shape
    tiles, rest = divmod(args[10].shape[1], LANE)
    fits = (
        n_sp % 2 == 0
        and n_sp % 4 == 0
        and n_tp == 4
        and rest == 0
        and 0 < tiles - n_sp
        and 2 * (tiles - n_sp) <= n_sp
        and tokens == LANE
        and width == 2 * DH
        and n_sp * tokens <= 1024
    )
    if fits:
        return fast_layer(n_sp, n_tp, *args)
    return per_device(*args)


def solution(mesh):
    return jax.shard_map(
        functools.partial(choose, mesh.shape["sp"], mesh.shape["tp"]),
        mesh=mesh,
        in_specs=(
            P("sp", "tp"),
            P("sp", "tp"),
            P("sp", "tp"),
            P("sp", "tp"),
            P("sp", "tp"),
            P(None, "tp", "sp"),
            P(None, "tp", "sp"),
            P("tp"),
            P("tp", None),
            P("tp"),
            P("sp", "tp"),
            P("sp", "tp"),
            P(None, "tp"),
            P("tp", "sp"),
        ),
        out_specs=P("sp", "tp"),
        check_vma=False,
    )
```

```python
import functools

import jax
import jax.numpy as jnp
from jax import lax
from jax.experimental import pallas as pl
from jax.experimental.pallas import tpu as pltpu
from jax.sharding import PartitionSpec as P

D = 2048
DH = 128
BLOCK = 64


NEG = -1e30
EPS = 1e-06
HIGH = lax.Precision.HIGHEST


def entering(array, axis, combine, identity, reverse):
    size, here = (lax.axis_size(axis), lax.axis_index(axis))
    everything = jax.tree.map(lambda part: lax.all_gather(part, axis), array)
    start = jax.tree.map(
        lambda part, zero: jnp.broadcast_to(jnp.asarray(zero, part.dtype), part.shape),
        array,
        identity,
    )

    def lap(k, before):
        at = size - 1 - k if reverse else k
        reached = at > here if reverse else at < here
        new = combine(before, jax.tree.map(lambda part: part[at], everything))
        return jax.tree.map(lambda a, b: jnp.where(reached, a, b), new, before)

    return lax.fori_loop(0, size, lap, start)


def extended(array, sides, width):
    for axis, dim in sides:
        size, length = (lax.axis_size(axis), array.shape[dim])
        up = [(i, (i + 1) % size) for i in range(size - 1)]
        down = [(j, i) for i, j in up]
        last = lax.slice_in_dim(array, length - width, length, axis=dim)
        first = lax.slice_in_dim(array, 0, width, axis=dim)
        before = lax.ppermute(last, axis, up)
        after = lax.ppermute(first, axis, down)
        array = jnp.concatenate([before, array, after], axis=dim)
    return array


def heads_blocks(source, head_count):
    length = source.shape[0]
    shaped = source.astype(jnp.float32).reshape(length // BLOCK, BLOCK, head_count, DH)
    return shaped.transpose(2, 0, 1, 3)


def merge_states(earlier, later):
    c_early, m_early, b_early = earlier
    c_late, m_late, b_late = later
    m_new = jnp.maximum(b_late + m_early, m_late)
    c_new = (
        jnp.exp(b_late + m_early - m_new)[..., None, None] * c_early
        + jnp.exp(m_late - m_new)[..., None, None] * c_late
    )
    return (c_new, m_new, b_early + b_late)


def carry_step(carry, inputs):
    return (merge_states(carry, inputs), carry)


def block_terms(key_rows, values, log_in, log_forget):
    cumulative = jnp.cumsum(log_forget, axis=-1)
    block_end = cumulative[..., -1]
    weight_log = block_end[..., None] - cumulative + log_in
    m_local = jnp.max(weight_log, axis=-1)
    weights = jnp.exp(weight_log - m_local[..., None])
    c_local = jnp.einsum("hnsd,hnse->hnde", weights[..., None] * key_rows, values, precision=HIGH)
    return (cumulative, block_end, m_local, c_local)


def block_output(queries, key_rows, values, log_in, cumulative, c_start, m_start):
    a_log = cumulative + m_start[..., None]
    d_log = cumulative[..., :, None] - cumulative[..., None, :] + log_in[..., None, :]
    block_len = cumulative.shape[-1]
    lower_mask = jnp.arange(block_len)[:, None] >= jnp.arange(block_len)[None, :]
    d_log = jnp.where(lower_mask, d_log, -jnp.inf)
    m_row = jnp.maximum(a_log, jnp.max(d_log, axis=-1))
    decays = jnp.exp(d_log - m_row[..., None])
    carried = jnp.exp(a_log - m_row)
    scores = jnp.einsum("hntd,hnsd->hnts", queries, key_rows, precision=HIGH) * decays
    numerator = jnp.einsum("hnts,hnse->hnte", scores, values, precision=HIGH) + carried[
        ..., None
    ] * jnp.einsum("hntd,hnde->hnte", queries, c_start, precision=HIGH)
    return (numerator, m_row)


def single_direction(query, memory_keys, value, log_in, log_forget, reverse):
    head_count = query.shape[1] // DH
    nblocks = query.shape[0] // BLOCK
    queries = heads_blocks(query, head_count)
    key_rows = heads_blocks(memory_keys, head_count) * DH ** (-0.5)
    values = heads_blocks(value, head_count)
    log_in = log_in.reshape(head_count, nblocks, BLOCK)
    log_forget = log_forget.reshape(head_count, nblocks, BLOCK)
    cumulative, block_end, m_local, c_local = block_terms(key_rows, values, log_in, log_forget)
    identity = (
        jnp.zeros((head_count, DH, DH), jnp.float32),
        jnp.full((head_count,), NEG, jnp.float32),
        jnp.zeros((head_count,), jnp.float32),
    )
    totals, prefix = lax.scan(
        carry_step, identity, (jnp.moveaxis(c_local, 1, 0), m_local.T, block_end.T)
    )
    if reverse:
        incoming = entering(totals, "sp", merge_states, identity, True)
    else:
        incoming = entering(totals, "sp", merge_states, identity, False)
    starts = merge_states(tuple((member[None] for member in incoming)), prefix)
    c_start = jnp.moveaxis(starts[0], 0, 1)
    m_start = starts[1].T
    numerator, m_row = block_output(queries, key_rows, values, log_in, cumulative, c_start, m_start)
    return (numerator.reshape(head_count, -1, DH), m_row.reshape(head_count, -1))


def per_device(
    resid,
    query,
    memory_keys,
    value,
    output_gate_logits,
    gate_preactivation,
    extra_forget_logs,
    head_norm_gain,
    output_weight,
    mixer_norm_gain,
    gate_up_weight,
    value_up_weight,
    convolution_weight,
    down_weight,
):
    tokens = query.shape[0]
    forward_numerator, forward_peak = single_direction(
        query,
        memory_keys,
        value,
        gate_preactivation[0],
        jax.nn.log_sigmoid(gate_preactivation[1]) + extra_forget_logs[0],
        False,
    )
    backward_numerator, backward_peak = single_direction(
        jnp.flip(query, 0),
        jnp.flip(memory_keys, 0),
        jnp.flip(value, 0),
        jnp.flip(gate_preactivation[2], -1),
        jnp.flip(jax.nn.log_sigmoid(gate_preactivation[3]) + extra_forget_logs[1], -1),
        True,
    )
    backward_numerator = jnp.flip(backward_numerator, 1)
    backward_peak = jnp.flip(backward_peak, 1)
    both_max = jnp.maximum(forward_peak, backward_peak)
    numerator = (
        jnp.exp(forward_peak - both_max)[..., None] * forward_numerator
        + jnp.exp(backward_peak - both_max)[..., None] * backward_numerator
    )
    normal_cell = numerator * lax.rsqrt(
        jnp.mean(numerator * numerator, axis=-1, keepdims=True) + EPS
    )
    cell = normal_cell.transpose(1, 0, 2).reshape(tokens, -1)
    cell = (
        cell
        * head_norm_gain.astype(jnp.float32)
        * jax.nn.sigmoid(output_gate_logits.astype(jnp.float32))
    ).astype(jnp.bfloat16)
    partial_proj = jnp.dot(cell, output_weight, preferred_element_type=jnp.float32)
    stream = (
        resid.astype(jnp.float32)
        + lax.psum_scatter(
            partial_proj.astype(jnp.bfloat16), "tp", scatter_dimension=1, tiled=True
        ).astype(jnp.float32)
    ).astype(jnp.bfloat16)
    stream_f = stream.astype(jnp.float32)
    squares = lax.psum(jnp.sum(stream_f * stream_f, axis=1), "tp")
    normed_own = (
        stream_f * lax.rsqrt(squares / D + EPS)[:, None] * mixer_norm_gain.astype(jnp.float32)
    ).astype(jnp.bfloat16)
    normed = lax.all_gather(normed_own, "tp", axis=1, tiled=True)
    gate_sum = jnp.dot(
        normed,
        lax.all_gather(gate_up_weight, "sp", axis=0, tiled=True),
        preferred_element_type=jnp.float32,
    )
    value_sum = jnp.dot(
        normed,
        lax.all_gather(value_up_weight, "sp", axis=0, tiled=True),
        preferred_element_type=jnp.float32,
    )
    gate_mix = gate_sum.astype(jnp.bfloat16)
    value_mix = value_sum.astype(jnp.bfloat16)
    padded = extended(gate_mix, (("sp", 0),), 1)
    padded_f = padded.astype(jnp.float32)
    convolved = (
        convolution_weight[0] * padded_f[:-2]
        + convolution_weight[1] * padded_f[1:-1]
        + convolution_weight[2] * padded_f[2:]
    )
    hidden = (jax.nn.gelu(convolved) * value_mix.astype(jnp.float32)).astype(jnp.bfloat16)
    down_term = jnp.dot(
        hidden,
        lax.all_gather(down_weight, "sp", axis=1, tiled=True),
        preferred_element_type=jnp.float32,
    )
    mixer_out = lax.psum_scatter(
        down_term.astype(jnp.bfloat16), "tp", scatter_dimension=1, tiled=True
    ).astype(jnp.float32)
    return (stream.astype(jnp.float32) + mixer_out).astype(jnp.bfloat16)


LANE = 128
MESH = pl.DeviceIdType.MESH
F32 = jnp.float32
BF16 = jnp.bfloat16


def remote(src, dst, send, recv, sp, tp):
    return pltpu.make_async_remote_copy(
        src_ref=src,
        dst_ref=dst,
        send_sem=send,
        recv_sem=recv,
        device_id=(sp, tp),
        device_id_type=MESH,
    )


def nt_dot(a, b, precision=None):
    return lax.dot_general(
        a, b, (((1,), (1,)), ((), ())), precision=precision, preferred_element_type=F32
    )


def layer_kernel(
    n_sp,
    n_tp,
    resid,
    query,
    keys,
    value,
    gate_logits,
    gates,
    extra_logs,
    head_gain,
    out_w,
    mixer_gain,
    gate_w,
    value_w,
    taps,
    down_w,
    out,
    k_all,
    v_all,
    g_own,
    g_all,
    lf_own,
    wo_all,
    taps_all,
    gain_own,
    gain_all,
    w_up,
    w_down,
    cell_own,
    cell_all,
    stream_own,
    x_all,
    gate_buf,
    value_buf,
    halo,
    hidden_buf,
    part,
    part_sum,
    part_in,
    sum_in,
    z_out,
    r_all,
    k_sem,
    v_sem,
    g_sem,
    wo_sem,
    taps_sem,
    gain_sem,
    wg_sem,
    wv_sem,
    wd_sem,
    xg_sem,
    xv_sem,
    xd_sem,
    fwd_sem,
    cell_sem,
    x_send,
    x_fwd,
    x_relay,
    x_recv,
    halo_sem,
    p_sem,
    q_sem,
    z_send,
    r_recv,
    local_sem,
    local_x,
):
    s, t = (lax.axis_index("sp"), lax.axis_index("tp"))
    core = lax.rem(t, 2)
    pair = t // 2
    partner = t + 1 - 2 * core
    n_pair = n_tp // 2
    tokens = query.shape[0]
    width = query.shape[1]
    features = resid.shape[1]
    depth = gate_w.shape[0]
    cols = down_w.shape[1]
    heads = width // DH
    tiles = gate_w.shape[1] // LANE
    extras = tiles - n_sp
    half = n_sp // 2
    my_half = s // half
    model = features * n_tp
    z, y = (s // 2, lax.rem(s, 2))
    layers = half // 2
    x_side = (s, 2 * (1 - pair) + core)
    y_side = (2 * z + 1 - y, t)

    def loop(low, high, body):
        def step(i, carry):
            body(i)
            return carry

        lax.fori_loop(low, high, step, 0)

    rows = lambda i: pl.ds(pl.multiple_of(i * tokens, tokens), tokens)
    lanes = lambda i, size: pl.ds(pl.multiple_of(i * size, LANE), size)
    drows = lambda i: pl.ds(pl.multiple_of(i * depth, depth), depth)
    trows = lambda i: pl.ds(pl.multiple_of(i * LANE, LANE), LANE)

    def kv_copies(d):
        to = (lax.rem(2 * d + s, n_sp), t)
        return kv_pair((keys, value), s, d, to)

    def kv_side():
        return kv_pair((keys, value), s, 0, y_side)

    def kv_relay(d):
        source = lax.rem(s - 2 * d + n_sp, n_sp)
        at = rows(source)
        return kv_pair((k_all.at[at, :], v_all.at[at, :]), source, half + d, y_side)

    def kv_pair(refs, source, at, to):
        return (
            remote(refs[0], k_all.at[rows(source), :], k_sem.at[0, at], k_sem.at[1, at], *to),
            remote(refs[1], v_all.at[rows(source), :], v_sem.at[0, at], v_sem.at[1, at], *to),
        )

    def g_copy(d):
        to = lax.rem(s + d, n_sp)
        return remote(g_own, g_all.at[s], g_sem.at[0, d], g_sem.at[1, d], to, t)

    def wo_copy(e):
        to = lax.rem(t + e, n_tp)
        return remote(
            out_w.at[:, lanes(to, features)],
            wo_all.at[pl.ds(pl.multiple_of(t * width, width), width), :],
            wo_sem.at[0, e],
            wo_sem.at[1, e],
            s,
            to,
        )

    def gain_copy(e):
        to = lax.rem(t + e, n_tp)
        return remote(
            gain_own, gain_all.at[:, lanes(t, features)], gain_sem.at[0, e], gain_sem.at[1, e], s, to
        )

    def taps_copy():
        return remote(taps, taps_all.at[core], taps_sem.at[0], taps_sem.at[1], s, partner)

    def tile_ends(tile, slot):
        return (
            (gate_w.at[:, lanes(tile, LANE)], w_up.at[slot, drows(s), pl.ds(0, LANE)]),
            (value_w.at[:, lanes(tile, LANE)], w_up.at[slot, drows(s), pl.ds(LANE, LANE)]),
            (down_w.at[trows(tile), :], w_down.at[trows(slot), lanes(s, cols)]),
        )

    def weight_copies(d):
        to = lax.rem(s + d, n_sp)
        sems = (wg_sem, wv_sem, wd_sem)
        return tuple(
            remote(a, b, sem.at[0, d], sem.at[1, d], to, t)
            for (a, b), sem in zip(tile_ends(to, core), sems)
        )

    def extra_copies(e, source):
        to = e + extras * core
        sems = (xg_sem, xv_sem, xd_sem)
        return tuple(
            remote(a, b, sem.at[0, e], sem.at[1, source], to, t)
            for (a, b), sem in zip(tile_ends(n_sp + e, 2), sems)
        )

    def local_copies():
        pairs = (
            (keys, k_all.at[rows(s), :]),
            (value, v_all.at[rows(s), :]),
            (out_w.at[:, lanes(t, features)],
             wo_all.at[pl.ds(pl.multiple_of(t * width, width), width), :]),
        ) + tile_ends(s, core)
        return tuple(
            pltpu.make_async_copy(a, b, local_sem.at[i]) for i, (a, b) in enumerate(pairs)
        )

    def local_extra(e):
        return tuple(
            pltpu.make_async_copy(a, b, local_x.at[i])
            for i, (a, b) in enumerate(tile_ends(n_sp + e, 2))
        )

    barrier = pltpu.get_barrier_semaphore()

    def greet(to_s, to_t):
        pl.semaphore_signal(barrier, inc=1, device_id=(to_s, to_t), device_id_type=MESH)

    loop(1, n_sp, lambda d: greet(lax.rem(s + d, n_sp), t))
    loop(1, n_tp, lambda e: greet(s, lax.rem(t + e, n_tp)))
    loop(1, half, lambda d: greet(2 * lax.rem(z + d, half) + y, partner))
    pl.semaphore_wait(barrier, n_sp + n_tp + half - 3)

    def start_kv(d):
        for copy in kv_copies(d):
            copy.start()

    for copy in kv_side():
        copy.start()
    loop(1, half, start_kv)
    for copy in local_copies():
        copy.start()

    def log_sigmoid(x):
        return jnp.minimum(x, 0.0) - jnp.log1p(jnp.exp(-jnp.abs(x)))

    lf_own[...] = jnp.zeros_like(lf_own)
    lf_own[0:heads, :] = log_sigmoid(gates[1]) + extra_logs[0]
    lf_own[heads : 2 * heads, :] = log_sigmoid(gates[3]) + extra_logs[1]
    lf = lf_own[...]
    row_id = lax.broadcasted_iota(jnp.int32, (tokens, tokens), 0)
    col_id = lax.broadcasted_iota(jnp.int32, (tokens, tokens), 1)
    upto = (row_id >= col_id).astype(F32)
    below = (row_id > col_id).astype(F32)
    row_incl = nt_dot(lf, upto, HIGH)
    row_excl = nt_dot(lf, below, HIGH)
    col_incl = nt_dot(upto, lf, HIGH)
    col_excl = nt_dot(below, lf, HIGH)
    total = jnp.broadcast_to(jnp.sum(lf, axis=1, keepdims=True), lf.shape)
    g_own[0:heads, :] = gates[0] - row_incl[0:heads]
    g_own[heads : 2 * heads, :] = gates[2] + row_excl[heads : 2 * heads]
    g_own[2 * heads : 4 * heads, :] = total[0 : 2 * heads]
    gain_own[...] = jnp.broadcast_to(mixer_gain[...].astype(F32).reshape(1, features), gain_own.shape)
    g_all[s] = g_own[...]
    gain_all[:, lanes(t, features)] = gain_own[...]
    taps_all[core] = taps[...]
    loop(1, n_sp, lambda d: g_copy(d).start())

    def start_tp(e):
        wo_copy(e).start()
        gain_copy(e).start()

    loop(1, n_tp, start_tp)
    taps_copy().start()

    GATE, VALUE, DOWN = (slice(0, 1), slice(1, 2), slice(2, 3))
    KINDS = (GATE, VALUE, DOWN)

    def start_weights(which):
        def body(d):
            for copy in weight_copies(d)[which]:
                copy.start()

        loop(1, n_sp, body)

    def start_extras(which):
        def body(e):
            @pl.when(e + extras * core != s)
            def _():
                for copy in extra_copies(e, s)[which]:
                    copy.start()

            @pl.when(e + extras * core == s)
            def _():
                for copy in local_extra(e)[which]:
                    copy.start()

        loop(0, extras, body)

    start_weights(GATE)
    start_extras(GATE)

    def pass_kv(d):
        for copy, onward in zip(kv_copies(d), kv_relay(d)):
            copy.wait_recv()
            onward.start()

    loop(1, half, pass_kv)

    loop(1, n_sp, lambda d: g_copy(d).wait_recv())

    def wait_kv(d):
        for copy in kv_relay(d):
            copy.wait_recv()

    for copy in local_copies()[:3]:
        copy.wait()
    g = [g_all[j] for j in range(n_sp)]
    diag_lower = row_id >= col_id
    diag_upper = row_id <= col_id
    logs, peaks = ([], [])
    for h in range(heads):
        acc = jnp.zeros((1, tokens), F32)
        rows_f = [None] * n_sp
        for j in reversed(range(n_sp)):
            acc = acc + jnp.where(j < s, g[j][2 * heads + h : 2 * heads + h + 1], 0.0)
            rows_f[j] = g[j][h : h + 1] + acc
        acc = jnp.zeros((1, tokens), F32)
        logs_h = []
        f_col = col_incl[:, h : h + 1]
        b_col = -col_excl[:, heads + h : heads + h + 1]
        peak = jnp.full((tokens, 1), NEG, F32)
        for j in range(n_sp):
            row_b = g[j][heads + h : heads + h + 1] + acc
            acc = acc + jnp.where(j >= s, g[j][3 * heads + h : 3 * heads + h + 1], 0.0)
            fwd = jnp.where(jnp.logical_or(j < s, jnp.logical_and(j == s, diag_lower)), f_col + rows_f[j], NEG)
            bwd = jnp.where(jnp.logical_or(j > s, jnp.logical_and(j == s, diag_upper)), b_col + row_b, NEG)
            peak = jnp.maximum(peak, jnp.max(jnp.maximum(fwd, bwd), axis=1, keepdims=True))
            logs_h.append((fwd, bwd))
        peaks.append(peak)
        logs.append(
            jnp.concatenate([jnp.exp(f - peak) + jnp.exp(b - peak) for f, b in logs_h], axis=1)
        )
    for copy in kv_side():
        copy.wait_recv()
    loop(1, half, wait_kv)
    head_row = head_gain[...].astype(F32).reshape(1, width)
    for h in range(heads):
        lane = slice(h * DH, (h + 1) * DH)
        scores = nt_dot(query[:, lane], k_all[:, lane]) * DH ** (-0.5)
        weighted = (scores * logs[h]).astype(BF16)
        numer = jnp.dot(weighted, v_all[:, lane], preferred_element_type=F32)
        scale = lax.rsqrt(jnp.mean(numer * numer, axis=1, keepdims=True) + EPS)
        gated = (
            numer * scale * head_row[:, lane]
            * jax.nn.sigmoid(gate_logits[:, lane].astype(F32))
        )
        cell_own[:, lane] = gated.astype(BF16)

    def cell_copy(e):
        to = lax.rem(t + e, n_tp)
        return remote(cell_own, cell_all.at[t], cell_sem.at[0, e], cell_sem.at[1, e], s, to)

    loop(1, n_tp, lambda e: cell_copy(e).start())
    cell_all[t] = cell_own[...]

    def wait_tp(e):
        wo_copy(e).wait_recv()
        gain_copy(e).wait_recv()
        cell_copy(e).wait_recv()

    loop(1, n_tp, wait_tp)
    projected = jnp.zeros((tokens, features), F32)
    for m in range(n_tp):
        piece = jnp.dot(
            cell_all[m], wo_all[m * width : (m + 1) * width, :], preferred_element_type=F32
        )
        projected = projected + piece.astype(BF16).astype(F32)
    stream_own[...] = (resid[...].astype(F32) + projected).astype(BF16)

    def wait_weights(which):
        def body(d):
            for copy in weight_copies(d)[which]:
                copy.wait_recv()

        loop(1, n_sp, body)

    owner = jnp.logical_and(s >= extras * core, s < extras * (core + 1))
    other_owner = jnp.logical_and(s >= extras * (1 - core), s < extras * (2 - core))

    def forward_copy(slot, down):
        if down == 2:
            ref = w_down.at[trows(slot), :]
        else:
            ref = w_up.at[slot, :, pl.ds(down * LANE, LANE)]
        at = down + (3 if isinstance(slot, int) else 0)
        return remote(ref, ref, fwd_sem.at[0, at], fwd_sem.at[1, at], s, partner)

    def pass_on(down):
        which = KINDS[down]
        wait_weights(which)
        for copy in local_copies()[3:][which]:
            copy.wait()
        forward_copy(core, down).start()

        @pl.when(owner)
        def _():
            def wait_extra(source):
                @pl.when(source != s)
                def _():
                    for copy in extra_copies(0, source)[which]:
                        copy.wait_recv()

            loop(0, n_sp, wait_extra)
            for copy in local_extra(0)[which]:
                copy.wait()
            forward_copy(2, down).start()

    def take_other(down):
        forward_copy(1 - core, down).wait_recv()

        @pl.when(other_owner)
        def _():
            forward_copy(2, down).wait_recv()

    place = lax.rem(s, half)

    def x_spot(zl, block_y, m):
        j = 2 * zl + block_y
        return x_all.at[j, :, lanes(m, features)], j * n_tp + m

    def own_shard(j, m):
        return jnp.logical_and(core * half + j == s, m == t)

    def x_copy(d):
        to_z = lax.rem(z + d, half)
        spot, index = x_spot(lax.rem(z, layers), y, t)
        to = (2 * to_z + y, 2 * pair + my_half)
        return remote(stream_own, spot, x_send.at[d], x_recv.at[index], *to)

    def x_pass(zl, block_y, m, send, to):
        spot, index = x_spot(zl, block_y, m)
        return remote(spot, spot, send, x_recv.at[index], *to)

    def stays(d):
        return jnp.logical_and(d == 0, core == my_half)

    def start_x(d):
        @pl.when(jnp.logical_not(stays(d)))
        def _():
            x_copy(d).start()

        @pl.when(stays(d))
        def _():
            x_all[place, :, lanes(t, features)] = stream_own[...]

    loop(0, half, start_x)
    start_weights(VALUE)
    start_extras(VALUE)
    start_weights(DOWN)
    start_extras(DOWN)
    pass_on(0)

    def column(i):
        zl, m = (i // 2, 2 * pair + lax.rem(i, 2))

        @pl.when(jnp.logical_not(own_shard(2 * zl + y, m)))
        def _():
            x_pass(zl, y, m, x_fwd.at[0, i], x_side).wait_recv()

        x_pass(zl, y, m, x_fwd.at[0, i], x_side).start()
        x_pass(zl, y, m, x_fwd.at[1, i], y_side).start()

    loop(0, half, column)

    def relays(zl):
        return (
            x_pass(zl, y, 2 * (1 - pair), x_relay.at[0, zl], y_side),
            x_pass(zl, 1 - y, 2 * pair + 1, x_relay.at[1, zl], x_side),
        )

    def relay(zl):
        for copy in relays(zl):
            copy.wait_recv()
            copy.start()

    loop(0, layers, relay)

    @pl.when(s >= 2 * extras)
    def _():
        w_up[2] = jnp.zeros(w_up.shape[1:], BF16)
        w_down[2 * LANE :, :] = jnp.zeros((LANE, w_down.shape[1]), BF16)

    pass_on(1)
    take_other(0)
    take_other(1)

    def mix_block(i):
        zl, side = (lax.rem(i, layers), i // layers)
        j = 2 * zl + lax.rem(y + side, 2)
        for m in range(n_tp):
            mine = pair == m // 2
            if m % 2 == 0:
                seen = side == 0
            else:
                seen = mine

            @pl.when(jnp.logical_not(seen))
            def _(m=m):
                x_pass(zl, lax.rem(y + side, 2), m, x_relay.at[0, 0], y_side).wait_recv()

        x = x_all[j].astype(F32)
        squares = jnp.sum(x * x, axis=1, keepdims=True)
        normed = (x * lax.rsqrt(squares / model + EPS) * gain_all[0:1, :]).astype(BF16)
        for slot in range(3):
            both = jnp.dot(normed, w_up[slot], preferred_element_type=F32).astype(BF16)
            lane = slice(slot * LANE, (slot + 1) * LANE)
            gate_buf[rows(j), lane] = both[:, :LANE]
            value_buf[rows(j), lane] = both[:, LANE:]

    loop(0, half, mix_block)

    count = half * tokens
    edge = halo.shape[0]

    def halo_copy():
        start = pl.multiple_of((1 - core) * (count - edge), edge)
        return remote(
            gate_buf.at[pl.ds(start, edge), :], halo, halo_sem.at[0], halo_sem.at[1], s, partner
        )

    halo_copy().start()
    pass_on(2)
    taps_copy().wait_recv()
    halo_copy().wait_recv()
    extra_core = jnp.where(s < extras, 0, 1)
    extra_tile = jnp.minimum(n_sp + s - extras * extra_core, tiles - 1)
    slots = ((0, s), (1, s), (extra_core, extra_tile))
    pos = lax.broadcasted_iota(jnp.int32, (count, LANE), 0)
    for slot, (block, tile) in enumerate(slots):
        lane = slice(slot * LANE, (slot + 1) * LANE)
        tap = taps_all[block, :, lanes(tile, LANE)]
        g_mid = gate_buf[:, lane].astype(F32)
        edge_rows = halo[:, lane].astype(F32)
        before = jnp.where(core == 1, edge_rows[edge - 1 : edge], 0.0)
        after = jnp.where(core == 0, edge_rows[0:1], 0.0)
        g_prev = jnp.where(pos == 0, before, pltpu.roll(g_mid, 1, 0))
        g_next = jnp.where(pos == count - 1, after, pltpu.roll(g_mid, count - 1, 0))
        conv = tap[0:1] * g_prev + tap[1:2] * g_mid + tap[2:3] * g_next
        mixed = jax.nn.gelu(conv) * value_buf[:, lane].astype(F32)
        hidden_buf[:, lane] = mixed.astype(BF16)

    take_other(2)

    def product(j, m):
        return jnp.dot(
            hidden_buf[rows(j), :], w_down[:, lanes(m, features)], preferred_element_type=F32
        )

    def first_copies(i):
        return tuple(
            remote(part.at[k, i], part_in.at[k, i], p_sem.at[0, k, i], p_sem.at[1, k, i], *to)
            for k, to in enumerate((x_side, y_side))
        )

    def second_copies(zl):
        return tuple(
            remote(
                part_sum.at[k, zl], sum_in.at[k, zl], q_sem.at[0, k, zl], q_sem.at[1, k, zl], *to
            )
            for k, to in enumerate((y_side, x_side))
        )

    def z_copy(k, zl):
        to = (2 * (core * layers + zl) + y, 2 * pair + k)
        mine = jnp.logical_and(to[0] == s, to[1] == t)
        return mine, remote(z_out.at[k, zl], r_all.at[z], z_send.at[k, zl], r_recv.at[z], *to)

    def first_trip(n):
        zl, late = (lax.rem(n, layers), n // layers)
        by = lax.rem(1 - y + late, 2)
        bx = lax.rem(1 - pair + late, 2)
        i_x, i_y = (2 * zl + by, 2 * zl + bx)
        part[0, i_x] = product(2 * zl + by, 2 * (1 - pair)).astype(BF16)
        first_copies(i_x)[0].start()
        part[1, i_y] = product(2 * zl + 1 - y, 2 * bx + 1).astype(BF16)
        first_copies(i_y)[1].start()

    loop(0, half, first_trip)

    def second_trip(zl):
        i_x, i_y = (2 * zl + 1 - y, 2 * zl + 1 - pair)
        own = product(2 * zl + 1 - y, 2 * pair)
        first_copies(i_x)[0].wait_recv()
        part_sum[0, zl] = (own + part_in[0, i_x].astype(F32)).astype(BF16)
        second_copies(zl)[0].start()
        own = product(2 * zl + y, 2 * (1 - pair) + 1)
        first_copies(i_y)[1].wait_recv()
        part_sum[1, zl] = (own + part_in[1, i_y].astype(F32)).astype(BF16)
        second_copies(zl)[1].start()

    loop(0, layers, second_trip)

    def third_trip(zl):
        for k, i in enumerate((2 * zl + y, 2 * zl + pair)):
            own = product(2 * zl + y, 2 * pair + k)
            first_copies(i)[k].wait_recv()
            own = own + part_in[k, i].astype(F32)
            second_copies(zl)[k].wait_recv()
            result = (own + sum_in[k, zl].astype(F32)).astype(BF16)
            z_out[k, zl] = result
            mine, copy = z_copy(k, zl)

            @pl.when(jnp.logical_not(mine))
            def _():
                copy.start()

            @pl.when(mine)
            def _():
                r_all[z] = result

    loop(0, layers, third_trip)

    out_sum = jnp.zeros((tokens, features), F32)
    for i in range(half):

        @pl.when(jnp.logical_not(jnp.logical_and(core == my_half, z == i)))
        def _(i=i):
            remote(z_out.at[0, 0], r_all.at[i], z_send.at[0, 0], r_recv.at[i], *y_side).wait_recv()

        out_sum = out_sum + r_all[i].astype(F32)
    out[...] = (stream_own[...].astype(F32) + out_sum).astype(BF16)

    def sent_sp(d):
        for copy in (g_copy(d),) + weight_copies(d):
            copy.wait_send()

    loop(1, n_sp, sent_sp)
    for copy in kv_side():
        copy.wait_send()

    def sent_kv(d):
        for copy in kv_copies(d) + kv_relay(d):
            copy.wait_send()

    loop(1, half, sent_kv)

    def sent_tp(e):
        wo_copy(e).wait_send()
        gain_copy(e).wait_send()
        cell_copy(e).wait_send()

    loop(1, n_tp, sent_tp)
    taps_copy().wait_send()

    def sent_extra(e):
        @pl.when(e + extras * core != s)
        def _():
            for copy in extra_copies(e, s):
                copy.wait_send()

    loop(0, extras, sent_extra)

    def sent_x(d):
        @pl.when(jnp.logical_not(stays(d)))
        def _():
            x_copy(d).wait_send()

        for k, to in enumerate((x_side, y_side)):
            x_pass(d // 2, y, 2 * pair + lax.rem(d, 2), x_fwd.at[k, d], to).wait_send()
        for copy in first_copies(d):
            copy.wait_send()

    loop(0, half, sent_x)

    def sent_layer(zl):
        for copy in relays(zl) + second_copies(zl):
            copy.wait_send()
        for k in range(2):
            mine, copy = z_copy(k, zl)

            @pl.when(jnp.logical_not(mine))
            def _(copy=copy):
                copy.wait_send()

    loop(0, layers, sent_layer)
    for down in range(3):
        forward_copy(core, down).wait_send()

    @pl.when(owner)
    def _():
        for down in range(3):
            forward_copy(2, down).wait_send()

    halo_copy().wait_send()


def fast_layer(n_sp, n_tp, *args):
    (resid, query, keys, value, gate_logits, gates, extra_logs, head_gain, out_w,
     mixer_gain, gate_w, value_w, taps, down_w) = args
    tokens, width = query.shape
    features = resid.shape[1]
    model = features * n_tp
    half = n_sp // 2
    n_pair = n_tp // 2
    hidden = 3 * LANE
    vmem = pl.BlockSpec(memory_space=pltpu.VMEM)
    anywhere = pl.BlockSpec(memory_space=pl.ANY)
    dma = pltpu.SemaphoreType.DMA
    spaces = [vmem, vmem, anywhere, anywhere, vmem, vmem, vmem, vmem, anywhere,
              vmem, anywhere, anywhere, vmem, anywhere]
    scratch = [
        pltpu.VMEM((n_sp * tokens, width), BF16),
        pltpu.VMEM((n_sp * tokens, width), BF16),
        pltpu.VMEM((8, tokens), F32),
        pltpu.VMEM((n_sp, 8, tokens), F32),
        pltpu.VMEM((8, tokens), F32),
        pltpu.VMEM((n_tp * width, features), BF16),
        pltpu.VMEM((2,) + taps.shape, F32),
        pltpu.VMEM((8, features), F32),
        pltpu.VMEM((8, model), F32),
        pltpu.VMEM((3, model, 2 * LANE), BF16),
        pltpu.VMEM((hidden, model), BF16),
        pltpu.VMEM((tokens, width), BF16),
        pltpu.VMEM((n_tp, tokens, width), BF16),
        pltpu.VMEM((tokens, features), BF16),
        pltpu.VMEM((half, tokens, model), BF16),
        pltpu.VMEM((half * tokens, hidden), BF16),
        pltpu.VMEM((half * tokens, hidden), BF16),
        pltpu.VMEM((16, hidden), BF16),
        pltpu.VMEM((half * tokens, hidden), BF16),
        pltpu.VMEM((2, half, tokens, features), BF16),
        pltpu.VMEM((2, half // 2, tokens, features), BF16),
        pltpu.VMEM((2, half, tokens, features), BF16),
        pltpu.VMEM((2, half // 2, tokens, features), BF16),
        pltpu.VMEM((2, half // 2, tokens, features), BF16),
        pltpu.VMEM((half, tokens, features), BF16),
        dma((2, n_sp)),
        dma((2, n_sp)),
        dma((2, n_sp)),
        dma((2, n_tp)),
        dma((2,)),
        dma((2, n_tp)),
        dma((2, n_sp)),
        dma((2, n_sp)),
        dma((2, n_sp)),
        dma((2, n_sp)),
        dma((2, n_sp)),
        dma((2, n_sp)),
        dma((2, n_sp)),
        dma((2, n_tp)),
        dma((half,)),
        dma((2, half)),
        dma((2, half // 2)),
        dma((half * n_tp,)),
        dma((2,)),
        dma((2, 2, half)),
        dma((2, 2, half // 2)),
        dma((2, half // 2)),
        dma((half,)),
        dma((6,)),
        dma((3,)),
    ]
    return pl.pallas_call(
        functools.partial(layer_kernel, n_sp, n_tp),
        out_shape=jax.ShapeDtypeStruct((tokens, features), BF16),
        in_specs=spaces,
        out_specs=vmem,
        scratch_shapes=scratch,
        compiler_params=pltpu.CompilerParams(has_side_effects=True, collective_id=0, vmem_limit_bytes=60 * 2**20),
    )(resid, query, keys, value, gate_logits, gates, extra_logs, head_gain, out_w,
      mixer_gain, gate_w, value_w, taps, down_w)


def choose(n_sp, n_tp, *args):
    tokens, width = args[1].shape
    tiles, rest = divmod(args[10].shape[1], LANE)
    fits = (
        n_sp % 2 == 0
        and n_sp % 4 == 0
        and n_tp == 4
        and rest == 0
        and 0 < tiles - n_sp
        and 2 * (tiles - n_sp) <= n_sp
        and tokens == LANE
        and width == 2 * DH
        and n_sp * tokens <= 1024
    )
    if fits:
        return fast_layer(n_sp, n_tp, *args)
    return per_device(*args)


def solution(mesh):
    return jax.shard_map(
        functools.partial(choose, mesh.shape["sp"], mesh.shape["tp"]),
        mesh=mesh,
        in_specs=(
            P("sp", "tp"),
            P("sp", "tp"),
            P("sp", "tp"),
            P("sp", "tp"),
            P("sp", "tp"),
            P(None, "tp", "sp"),
            P(None, "tp", "sp"),
            P("tp"),
            P("tp", None),
            P("tp"),
            P("sp", "tp"),
            P("sp", "tp"),
            P(None, "tp"),
            P("tp", "sp"),
        ),
        out_specs=P("sp", "tp"),
        check_vma=False,
    )
```
